1024 devices in a mesh: kv: 256 (over z, y, core), tp: 4 (over x).
Axes of the slice: x: 4, y: 8, z: 16, core: 2. Of those that a mesh axis runs over, the one named last changes fastest.
Arguments:
- layer_input: bfloat16 [49152, 2048], P('kv', 'tp'), may hold values from -0.109375 to 0.109375
- queries: bfloat16 [49152, 1024], P('kv', 'tp'), may hold values from -6 to 6
- keys: bfloat16 [49152, 256], P('kv', 'tp'), may hold values from -6 to 6
- values: bfloat16 [49152, 256], P('kv', 'tp'), may hold values from -6 to 6
- attn_out: bfloat16 [49152, 1024], P('kv', 'tp'), may hold values from -1.25 to 1.25
- grad_out: bfloat16 [49152, 1024], P('kv', 'tp'), may hold values from -128 to 128
- log_sum: float32 [49152, 16], P('kv', 'tp'), may hold values from 6 to 7.5
- chosen: int32 [768, 8], replicated, may hold values from -1 to 767, as said below
Outputs:
- grad_queries: bfloat16 [49152, 1024], P('kv', 'tp')
- grad_keys: bfloat16 [49152, 256], P('kv', 'tp')
- grad_values: bfloat16 [49152, 256], P('kv', 'tp')
- grad_weight: float32 [2048, 1024], P('kv', 'tp')
The draws below stay inside these ranges and needn't reach their ends.
Inputs may be any that keep to these rules, and one draw needn't show every extreme that they name: Write R = 3 and call positions [s * 192, (s + 1) * 192) segment s. For query block b in segment c = b // R and level l < 4, the entries chosen[b, 2 l + i] for i < 2 name 2 different key blocks of segment c - g_l, with g = 1, 32, 64, 128; all of them are -1 where c - g_l is negative.
All inputs are finite; a program needn't handle non-finite values.
Results may differ from the reference program's by a relative error of at most 0.0053.
Values may be sent and summed in bfloat16 or wider, within the bound.
A program may use at most 64 MiB of HBM per device.

```python
import jax
import jax.numpy as jnp
from jax import lax

D = 2048
HEADS = 16
KVH = 4
DH = 64
BLOCK = 64
PER = 2
LEVELS = 4
TOK_DEV = 192
TOKENS = 49152
TOPK = 8
HOP = 32


def draw_chosen(key, part):
    per_segment = TOK_DEV // BLOCK
    total_blocks = TOKENS // BLOCK
    distances = jnp.array([1, HOP, 2 * HOP, 4 * HOP], jnp.int32)
    block_ids = jnp.arange(total_blocks, dtype=jnp.int32)
    segment = block_ids // per_segment
    ranks = jax.random.randint(jax.random.fold_in(key, 17), (total_blocks, LEVELS, per_segment), 0, 1 << 20)
    ranks = ranks * per_segment + jnp.arange(per_segment, dtype=jnp.int32)
    unused, order = lax.top_k(ranks, PER)
    source = segment[:, None] - distances[None, :]
    picked = source[:, :, None] * per_segment + order.astype(jnp.int32)
    picked = jnp.where(source[:, :, None] >= 0, picked, -1)
    return picked.reshape(total_blocks, LEVELS * PER).astype(jnp.int32)


def spiked(values, own_key, source, target, parts, factor):
    def block_of(position):
        return (jnp.arange(values.shape[position]) // (values.shape[position] // parts)).reshape((-1,) + (1,) * (values.ndim - 1 - position))

    one_side = jax.random.permutation(own_key, parts)[block_of(target)]
    far = (block_of(target) + parts // 2) % parts
    return jnp.where((block_of(source) == one_side) | (block_of(source) == far), factor * values, values)


def level_of(own_key, extent, cuts, least, largest):
    gain, own = 1.0, jax.random.fold_in(own_key, 6)
    for axis_at, blocks in cuts:
        draws = jnp.exp(jax.random.uniform(jax.random.fold_in(own, axis_at), (blocks,), jnp.float32, least / len(cuts), largest / len(cuts)))
        gain = gain * jnp.repeat(draws, extent[axis_at] // blocks).reshape([-1 if axis == axis_at else 1 for axis in range(len(extent))])
    return gain


def centred(stream_key, dims, deviation, limit, cuts=(), held_as=jnp.bfloat16):
    result = deviation * jax.random.normal(stream_key, dims, jnp.float32)
    if cuts:
        result = result * level_of(stream_key, dims, cuts, -0.22, 0.18)
    return jnp.clip(result, -limit, limit).astype(held_as)


def heavy_noise(key, shape, spread, most, cuts, heavy, kind=jnp.bfloat16):
    entries = spread * jax.random.normal(key, shape, jnp.float32)
    if cuts:
        entries = entries * level_of(key, shape, cuts, -0.22, 0.18)
    return jnp.clip(spiked(entries, jax.random.fold_in(key, 3), *heavy), -most, most).astype(kind)


def setup_inputs(seed: int = 0) -> dict:
    streams_of = jax.random.split(jax.random.key(seed), 9)
    layer_input = heavy_noise(streams_of[0], (TOKENS, D), (TOKENS ** -0.5), 0.109375, ((0, 256), (1, 4)), (0, 1, 256, 6.0))
    queries = centred(streams_of[1], (TOKENS, HEADS * DH), 1.0, 6.0, ((0, 256), (1, 4)))
    keys = centred(streams_of[2], (TOKENS, KVH * DH), 1.0, 6.0, ((0, 256), (1, 4)))
    values = centred(streams_of[3], (TOKENS, KVH * DH), 1.0, 6.0, ((0, 256), (1, 4)))
    attn_out = centred(streams_of[4], (TOKENS, HEADS * DH), 0.2, 1.25, ((0, 256), (1, 4)))
    grad_out = centred(streams_of[5], (TOKENS, HEADS * DH), 24.0, 128.0, ((0, 256), (1, 4)))
    log_sum = jnp.clip(6.0 + 1.5 * jax.random.uniform(streams_of[6], (TOKENS, HEADS), jnp.float32) ** level_of(streams_of[6], (TOKENS, HEADS), ((0, 256), (1, 4)), -0.2, 0.2), 6.0, 7.5)
    chosen = draw_chosen(jax.random.fold_in(streams_of[8], 71), 0)
    return {"layer_input": layer_input, "queries": queries, "keys": keys, "values": values, "attn_out": attn_out, "grad_out": grad_out, "log_sum": log_sum, "chosen": chosen}


def pair_terms(query_blk, grad_blk, lse_blk, delta_blk, key_blk, value_blk, keep_mask, scale_value):
    query_f = query_blk.astype(jnp.float32)
    grad_f = grad_blk.astype(jnp.float32)
    key_f = key_blk.astype(jnp.float32)
    value_f = value_blk.astype(jnp.float32)
    scores = jnp.einsum('pbkge,pcke->pkgbc', query_f, key_f) * scale_value
    lse_cols = jnp.transpose(lse_blk, (0, 2, 3, 1))[..., None]
    delta_cols = jnp.transpose(delta_blk, (0, 2, 3, 1))[..., None]
    weights = jnp.where(keep_mask[:, None, None], jnp.exp(scores - lse_cols), jnp.float32(0.0))
    weights_low = lax.optimization_barrier(weights.astype(jnp.bfloat16)).astype(jnp.float32)
    dweights = jnp.einsum('pbkge,pcke->pkgbc', grad_f, value_f)
    dscores = lax.optimization_barrier((weights * (dweights - delta_cols)).astype(jnp.bfloat16)).astype(jnp.float32)
    grad_query = jnp.einsum('pkgbc,pcke->pbkge', dscores, key_f) * scale_value
    grad_key = jnp.einsum('pkgbc,pbkge->pcke', dscores, query_f) * scale_value
    grad_value = jnp.einsum('pkgbc,pbkge->pcke', weights_low, grad_f)
    return grad_query, grad_key, grad_value


def reference(layer_input, queries, keys, values, attn_out, grad_out, log_sum, chosen):
    total_rows = queries.shape[0]
    nblocks = total_rows // BLOCK
    group_size = HEADS // KVH
    scale_value = DH ** -0.5
    query_all = queries.reshape(nblocks, BLOCK, KVH, group_size, DH)
    grad_all = grad_out.reshape(nblocks, BLOCK, KVH, group_size, DH)
    delta_all = jnp.sum(grad_out.astype(jnp.float32).reshape(nblocks, BLOCK, KVH, group_size, DH)
                        * attn_out.astype(jnp.float32).reshape(nblocks, BLOCK, KVH, group_size, DH), axis=-1)
    lse_all = log_sum.reshape(nblocks, BLOCK, KVH, group_size)
    key_all = keys.reshape(nblocks, BLOCK, KVH, DH)
    value_all = values.reshape(nblocks, BLOCK, KVH, DH)
    causal = lax.broadcasted_iota(jnp.int32, (BLOCK, BLOCK), 0) >= lax.broadcasted_iota(jnp.int32, (BLOCK, BLOCK), 1)
    slot_ids = jnp.arange(TOPK + 1, dtype=jnp.int32)

    def one_block(carry, block_num):
        key_acc, value_acc = carry
        listed = chosen[block_num].astype(jnp.int32)
        targets = jnp.concatenate([block_num[None], listed]).astype(jnp.int32)
        is_live = targets >= 0
        safe_ids = jnp.where(is_live, targets, 0).astype(jnp.int32)
        keep_mask = jnp.where((slot_ids == 0)[:, None, None], causal[None], True) & is_live[:, None, None]
        count_pairs = TOPK + 1
        query_rep = jnp.broadcast_to(query_all[block_num][None], (count_pairs, BLOCK, KVH, group_size, DH))
        grad_rep = jnp.broadcast_to(grad_all[block_num][None], (count_pairs, BLOCK, KVH, group_size, DH))
        lse_rep = jnp.broadcast_to(lse_all[block_num][None], (count_pairs, BLOCK, KVH, group_size))
        delta_rep = jnp.broadcast_to(delta_all[block_num][None], (count_pairs, BLOCK, KVH, group_size))
        grad_query, grad_key, grad_value = pair_terms(query_rep, grad_rep, lse_rep, delta_rep,
                                                      key_all[safe_ids], value_all[safe_ids], keep_mask, scale_value)
        key_acc = key_acc.at[safe_ids].add(grad_key)
        value_acc = value_acc.at[safe_ids].add(grad_value)
        return (key_acc, value_acc), jnp.sum(grad_query, axis=0)

    zeros_acc = jnp.zeros((nblocks, BLOCK, KVH, DH), jnp.float32)
    (key_acc, value_acc), grad_blocks = lax.scan(one_block, (zeros_acc, zeros_acc),
                                                 jnp.arange(nblocks, dtype=jnp.int32))
    grad_queries = grad_blocks.reshape(total_rows, HEADS * DH).astype(jnp.bfloat16)
    grad_keys = key_acc.reshape(total_rows, KVH * DH).astype(jnp.bfloat16)
    grad_values = value_acc.reshape(total_rows, KVH * DH).astype(jnp.bfloat16)
    grad_weight = jnp.dot(layer_input.T, grad_queries, preferred_element_type=jnp.float32)
    return grad_queries, grad_keys, grad_values, grad_weight
```

```python
import functools

import jax
import jax.numpy as jnp
from jax import lax
from jax.experimental import pallas as pl
from jax.experimental.pallas import tpu as pltpu
from jax.sharding import Mesh
from jax.sharding import PartitionSpec as P

MESH = pl.DeviceIdType.MESH
F32 = jnp.float32
BF16 = jnp.bfloat16

DH = 64
BLOCK = 64
PER = 2
LEVELS = 4
LOG2E = 1.4426950408889634
BIG = 1e30
SIZES = {"z": 16, "y": 8, "c": 2, "x": 4}
KV = ("z", "y", "c")


def nt(a, b):
    return lax.dot_general(a, b, (((1,), (1,)), ((), ())), preferred_element_type=F32)


def tn(a, b):
    return lax.dot_general(a, b, (((0,), (0,)), ((), ())), preferred_element_type=F32)


def nn(a, b):
    return lax.dot_general(a, b, (((1,), (0,)), ((), ())), preferred_element_type=F32)


def kernel(
    x_hbm, q_hbm, kv_hbm, o_hbm, g_hbm, l_hbm, b_hbm,
    dq_ref, dk_ref, dv_ref, dw_ref,
    q_v, o_v, g_v, l_v, b_v, kv_v, x_v,
    w_v, lrow, drow, dqt, dkv_own, far, back, ret,
    xg, xt, dqa, ysend, yrecv, zsend, zrecv,
    load_sem, kv_ssem, kv_rsem, x_ssem, x_rsem, r_ssem, r_rsem, d_sem, y_ssem, y_rsem, z_ssem, z_rsem,
):
    nz, ny, nc, nx = (SIZES[a] for a in ("z", "y", "c", "x"))
    z, y, c, x = (lax.axis_index(a) for a in ("z", "y", "c", "x"))
    total = nz * ny * nc
    me = (z * ny + y) * nc + c

    def at(zz, yy, cc, xx):
        return {"z": zz, "y": yy, "c": cc, "x": xx}

    def segment(s):
        s = lax.rem(s + total, total)
        return at(s // (ny * nc), lax.rem(s // nc, ny), lax.rem(s, nc), x)

    def remote(src, dst, ssem, rsem, device):
        return pltpu.make_async_remote_copy(
            src_ref=src, dst_ref=dst, send_sem=ssem, recv_sem=rsem, device_id=device, device_id_type=MESH
        )

    half = nx // nc
    home = x // half
    slot = lax.rem(x, half) * nc + c

    loads = [
        pltpu.make_async_copy(s, d, load_sem.at[i])
        for i, (s, d) in enumerate(
            ((kv_hbm, kv_v), (q_hbm, q_v), (g_hbm, g_v), (o_hbm, o_v), (l_hbm, l_v), (b_hbm, b_v), (x_hbm, x_v))
        )
    ]
    for cp in loads:
        cp.start()

    barrier = pltpu.get_barrier_semaphore()

    def tell(device):
        pl.semaphore_signal(barrier, inc=1, device_id=device, device_id_type=MESH)

    for d in range(1, nx):
        for e in range(nc):
            tell(at(z, y, e, lax.rem(x + d, nx)))
    for d in range(1, ny):
        tell(at(z, lax.rem(y + d, ny), c, x))
    for d in range(1, nz):
        for e in range(nc):
            tell(at(lax.rem(z + d, nz), y, e, x))
    tell(at(z, y, 1 - c, x))
    tell(segment(me + 1))
    tell(segment(me - 1))
    peers = (nx - 1) * nc + (ny - 1) + (nz - 1) * nc + 3

    for cp in loads[1:]:
        cp.wait()
    loads[0].wait()
    tok = q_v.shape[0]
    nb = tok // BLOCK
    heads = q_v.shape[1] // DH
    low = lax.broadcasted_iota(jnp.int32, (BLOCK, 2 * DH), 1) < DH
    for b in range(nb):
        for hp in range(heads // 2):
            rows = pl.ds(b * BLOCK, BLOCK)
            cols = pl.ds(hp * 2 * DH, 2 * DH)
            qt = q_v[rows, cols].astype(F32) * (DH**-0.5)
            gt = g_v[rows, cols].astype(F32)
            qr = pltpu.roll(qt, DH, 1)
            gr = pltpu.roll(gt, DH, 1)
            for k, (qq, gg) in enumerate(((qt, gr), (qr, gt))):
                h = hp * 2 + k
                w_v[b, pl.ds(h * BLOCK, BLOCK), :] = jnp.where(low, qq, 0.0).astype(BF16)
                w_v[b, pl.ds((heads + h) * BLOCK, BLOCK), :] = jnp.where(low, 0.0, gg).astype(BF16)

    prod = g_v[...].astype(F32) * o_v[...].astype(F32)
    delta = jnp.sum(prod.T.reshape(heads, DH, tok), axis=1)
    lse = jnp.concatenate([l_v[...] * LOG2E, jnp.zeros((tok, 128 - heads), F32)], axis=1).T
    for b in range(nb):
        for h in range(heads):
            cols = pl.ds(h * BLOCK, BLOCK)
            drow[b, :, cols] = delta[h : h + 1, b * BLOCK : (b + 1) * BLOCK]
            lrow[b, :, cols] = lse[h : h + 1, b * BLOCK : (b + 1) * BLOCK]

    def tile(kv, b, l_of, keep):
        n = kv.shape[0] // BLOCK
        qw = w_v[b, pl.ds(0, heads * BLOCK), :]
        gw = w_v[b, pl.ds(heads * BLOCK, heads * BLOCK), :]
        scores = nt(kv, qw)
        dprobs = nt(kv, gw)
        dl = drow[b]
        ps, ds = [], []
        for k in range(n):
            rows = slice(k * BLOCK, (k + 1) * BLOCK)
            p = jnp.exp2(scores[rows] * LOG2E - l_of(k))
            if keep is not None:
                p = jnp.where(keep, p, 0.0)
            ps.append(p.astype(BF16))
            ds.append((p * (dprobs[rows] - dl)).astype(BF16))
        p = ps[0] if n == 1 else jnp.concatenate(ps, axis=0)
        d = ds[0] if n == 1 else jnp.concatenate(ds, axis=0)
        dkv = nn(d, qw) + nn(p, gw)
        return dkv, tn(kv[:, :DH], d)

    width = heads * BLOCK
    keep = lax.broadcasted_iota(jnp.int32, (BLOCK, width), 0) <= lax.rem(
        lax.broadcasted_iota(jnp.int32, (BLOCK, width), 1), BLOCK
    )

    def own(b, carry):
        rows = pl.ds(pl.multiple_of(b * BLOCK, BLOCK), BLOCK)
        dkv, dq = tile(kv_v[rows, :], b, lambda k: lrow[b], keep)
        dkv_own[rows, :] = dkv
        dqt[b] = dq
        return carry

    lax.fori_loop(0, nb, own, 0)

    pl.semaphore_wait(barrier, peers)

    reach = [1, total // 8, total // 4, total // 2]
    sends = []
    for l in (3, 2, 1, 0):
        cp = remote(kv_v, far.at[l], kv_ssem.at[l], kv_rsem.at[l], segment(me + reach[l]))
        cp.start()
        sends.append(cp)
    for d in range(1, nx):
        cp = remote(x_v, xg.at[slot], x_ssem.at[d], x_rsem.at[slot], at(z, y, home, lax.rem(x + d, nx)))
        cp.start()
        sends.append(cp)

    local_x = pltpu.make_async_copy(x_hbm, xg.at[slot], x_rsem.at[slot])
    cross_x = remote(x_v, xg.at[slot], x_ssem.at[0], x_rsem.at[slot], at(z, y, 1 - c, x))

    @pl.when(home == c)
    def _():
        local_x.start()

    @pl.when(home != c)
    def _():
        cross_x.start()

    for l in range(LEVELS):
        remote(kv_v, far.at[l], kv_ssem.at[l], kv_rsem.at[l], segment(me + reach[l])).wait_recv()

        def level(b, acc, l=l):
            kv = far[l]
            dkv, dq = tile(kv, b, lambda k: lrow[b] + b_v[b, pl.ds(l * 3 + k, 1), :], None)
            dqt[b] = dqt[b] + dq
            return acc + dkv

        acc = lax.fori_loop(0, nb, level, jnp.zeros((tok, 2 * DH), F32))
        back[l] = acc.astype(BF16)
        if l == LEVELS - 1:
            continue
        cp = remote(back.at[l], ret.at[l], r_ssem.at[l], r_rsem.at[l], segment(me - reach[l]))
        cp.start()
        sends.append(cp)

    for b in range(nb):
        t = (dqt[b] * (DH**-0.5)).T
        for h in range(heads):
            dqa[c, pl.ds(b * BLOCK, BLOCK), pl.ds(h * DH, DH)] = t[h * BLOCK : (h + 1) * BLOCK].astype(BF16)
    cross = remote(dqa.at[c], dqa.at[c], d_sem.at[0], d_sem.at[1], at(z, y, 1 - c, x))
    cross.start()
    l = LEVELS - 1
    cp = remote(back.at[l], ret.at[l], r_ssem.at[l], r_rsem.at[l], segment(me - reach[l]))
    cp.start()
    sends.append(cp)
    dq_ref[...] = dqa[c]

    for s in range(half * nc):
        pltpu.make_async_copy(x_hbm, xg.at[s], x_rsem.at[s]).wait()

    per = 128 // ny

    def flip(i, carry):
        s = i // 4
        k = lax.rem(i, 4)
        t = xg[s, :, pl.ds(pl.multiple_of(k * 128, 128), 128)].T
        row = pl.multiple_of(((s // nc) * 4 + k) * per, per)
        for yy in range(ny):
            xt[lax.rem(s, nc), yy, pl.ds(row, per), :] = t[yy * per : (yy + 1) * per]
        return carry

    lax.fori_loop(0, half * nc * 4, flip, 0)
    cross.wait()

    def chunk(yy):
        return nn(xt[0, yy], dqa[0]) + nn(xt[1, yy], dqa[1])

    order = sorted(range(1, ny), key=lambda d: -min(d, ny - d))
    for d in order:
        yy = lax.rem(y + d, ny)
        ysend[d - 1] = chunk(yy).astype(BF16)
        cp = remote(ysend.at[d - 1], yrecv.at[d - 1], y_ssem.at[d - 1], y_rsem.at[d - 1], at(z, yy, c, x))
        cp.start()
        sends.append(cp)
    acc = chunk(y)
    for d in order[::-1]:
        pltpu.make_async_copy(yrecv.at[d - 1], yrecv.at[d - 1], y_rsem.at[d - 1]).wait()
        acc = acc + yrecv[d - 1].astype(F32)
    zsend[...] = acc.astype(BF16).reshape(zsend.shape)

    nzl = nz // nc

    def spread(i, carry):
        zz = c * nzl + i // nc
        e = lax.rem(i, nc)
        self = jnp.logical_and(zz == z, e == c)

        @pl.when(jnp.logical_not(self))
        def _():
            remote(zsend.at[i], zrecv.at[z], z_ssem.at[i], z_rsem.at[z], at(zz, y, e, x)).start()

        @pl.when(self)
        def _():
            zrecv[z] = zsend[i]

        return carry

    lax.fori_loop(0, nzl * nc, spread, 0)

    total_kv = dkv_own[...]
    for l in range(LEVELS):
        pltpu.make_async_copy(ret.at[l], ret.at[l], r_rsem.at[l]).wait()
        total_kv = total_kv + ret[l].astype(F32)
    dk_ref[...] = total_kv[:, :DH].astype(BF16)
    dv_ref[...] = total_kv[:, DH:].astype(BF16)

    mine = z // nzl == c

    def gather(j, acc):
        @pl.when(jnp.logical_not(jnp.logical_and(j == z, mine)))
        def _():
            pltpu.make_async_copy(zrecv.at[j], zrecv.at[j], z_rsem.at[j]).wait()

        return acc + zrecv[j].astype(F32)

    dw_ref[...] = lax.fori_loop(0, nz, gather, jnp.zeros(dw_ref.shape, F32))

    for cp in sends:
        cp.wait_send()

    @pl.when(home != c)
    def _():
        cross_x.wait_send()

    def sent(i, carry):
        zz = c * nzl + i // nc
        e = lax.rem(i, nc)

        @pl.when(jnp.logical_not(jnp.logical_and(zz == z, e == c)))
        def _():
            remote(zsend.at[i], zrecv.at[z], z_ssem.at[i], z_rsem.at[z], at(zz, y, e, x)).wait_send()

        return carry

    lax.fori_loop(0, nzl * nc, sent, 0)


def shards(layer_input, queries, keys, values, attn_out, grad_out, log_sum, chosen):
    nz, ny, nc, nx = (SIZES[a] for a in ("z", "y", "c", "x"))
    total = nz * ny * nc
    me = lax.axis_index(KV)
    tok, qw = queries.shape
    nb = tok // BLOCK
    heads = qw // DH
    feats = layer_input.shape[1]
    rows_out = feats * nx // total
    kv = jnp.concatenate([keys, values], axis=1)
    reach = jnp.array([1, total // 8, total // 4, total // 2], jnp.int32)
    listed = lax.dynamic_slice(chosen, (me * nb, 0), (nb, LEVELS * PER)).reshape(nb, LEVELS, PER, 1)
    target = ((me - reach) * nb)[:, None] + jnp.arange(nb, dtype=jnp.int32)[None, :]
    hit = jnp.any((listed == target[None, :, None, :]) & (listed >= 0), axis=2)
    bias = jnp.where(hit, 0.0, BIG).astype(F32).reshape(nb, LEVELS * nb)
    bias = jnp.pad(bias, ((0, 0), (0, 16 - LEVELS * nb)))
    bias = jnp.broadcast_to(bias[:, :, None], (nb, 16, heads * BLOCK))

    half = nx // nc
    dma = pltpu.SemaphoreType.DMA
    vm = pltpu.VMEM
    anys = pl.BlockSpec(memory_space=pl.ANY)
    vmem = pl.BlockSpec(memory_space=pltpu.VMEM)
    chunk_rows = feats * half // ny
    return pl.pallas_call(
        kernel,
        out_shape=(
            jax.ShapeDtypeStruct((tok, qw), BF16),
            jax.ShapeDtypeStruct((tok, DH), BF16),
            jax.ShapeDtypeStruct((tok, DH), BF16),
            jax.ShapeDtypeStruct((rows_out, qw), F32),
        ),
        in_specs=[anys] * 7,
        out_specs=(vmem,) * 4,
        scratch_shapes=[
            vm((tok, qw), BF16), vm((tok, qw), BF16), vm((tok, qw), BF16), vm((tok, heads), F32),
            vm((nb, 16, heads * BLOCK), F32), vm((tok, 2 * DH), BF16), vm((tok, feats), BF16),
            vm((nb, 2 * heads * BLOCK, 2 * DH), BF16), vm((nb, 1, heads * BLOCK), F32), vm((nb, 1, heads * BLOCK), F32),
            vm((nb, DH, heads * BLOCK), F32), vm((tok, 2 * DH), F32),
            vm((LEVELS, tok, 2 * DH), BF16), vm((LEVELS, tok, 2 * DH), BF16), vm((LEVELS, tok, 2 * DH), BF16),
            vm((half * nc, tok, feats), BF16), vm((nc, ny, chunk_rows, tok), BF16), vm((nc, tok, qw), BF16),
            vm((ny - 1, chunk_rows, qw), BF16), vm((ny - 1, chunk_rows, qw), BF16),
            vm((nz, rows_out, qw), BF16), vm((nz, rows_out, qw), BF16),
            dma((7,)), dma((LEVELS,)), dma((LEVELS,)), dma((nx,)), dma((half * nc,)), dma((LEVELS,)), dma((LEVELS,)),
            dma((2,)), dma((ny - 1,)), dma((ny - 1,)), dma((nz,)), dma((nz,)),
        ],
        compiler_params=pltpu.CompilerParams(collective_id=0, has_side_effects=True, vmem_limit_bytes=48 * 1024 * 1024),
        name="whole",
    )(layer_input, queries, kv, attn_out, grad_out, log_sum, bias)


def solution(mesh):
    torus = Mesh(
        mesh.devices.reshape(SIZES["z"], SIZES["y"], SIZES["c"], SIZES["x"]), ("z", "y", "c", "x")
    )
    spec = P(KV, "x")
    return jax.shard_map(
        shards,
        mesh=torus,
        in_specs=(spec,) * 7 + (P(),),
        out_specs=(spec,) * 4,
        check_vma=False,
    )
```

```python
import functools

import jax
import jax.numpy as jnp
from jax import lax
from jax.experimental import pallas as pl
from jax.experimental.pallas import tpu as pltpu
from jax.sharding import Mesh
from jax.sharding import PartitionSpec as P

MESH = pl.DeviceIdType.MESH
F32 = jnp.float32
BF16 = jnp.bfloat16

DH = 64
BLOCK = 64
PER = 2
LEVELS = 4
LOG2E = 1.4426950408889634
BIG = 1e30
SIZES = {"z": 16, "y": 8, "c": 2, "x": 4}
KV = ("z", "y", "c")


def nt(a, b):
    return lax.dot_general(a, b, (((1,), (1,)), ((), ())), preferred_element_type=F32)


def tn(a, b):
    return lax.dot_general(a, b, (((0,), (0,)), ((), ())), preferred_element_type=F32)


def nn(a, b):
    return lax.dot_general(a, b, (((1,), (0,)), ((), ())), preferred_element_type=F32)


def groups_of(half):
    out, at, n = [(0, 1)], 1, 1
    while at < half:
        out.append((at, n))
        at, n = at + n, n * 2
    return out


def kernel(
    x_hbm, q_hbm, k_hbm, v_hbm, o_hbm, g_hbm, l_hbm, ch_hbm,
    dq_ref, dk_ref, dv_ref, dw_ref,
    q_v, o_v, g_v, l_v, ch_v, kt_v, vt_v, kv_v,
    w_v, lrow, drow, dqt, dkv_own, far, back, ret,
    xg, xt, *rest,
):
    nz, ny, nc, nx = (SIZES[a] for a in ("z", "y", "c", "x"))
    half = nz // 2
    groups = groups_of(half)
    ng = len(groups)
    ys, yr = rest[:ng], rest[ng : 2 * ng]
    (pe, pr, ys2, yr2, zs, zr, load_sem, kv_s, kv_r, x_s, x_r, r_s, r_r, y_s, y_r, p_s, p_r, y2_s, y2_r, z_s, z_r,
     near_sem) = rest[2 * ng :]
    z, y, c, x = (lax.axis_index(a) for a in ("z", "y", "c", "x"))
    total = nz * ny * nc
    me = (z * ny + y) * nc + c
    seat = y * nc + c
    seats = ny * nc
    step = nz // 4

    def at(zz, yy, cc, xx):
        return {"z": zz, "y": yy, "c": cc, "x": xx}

    def zmate(d):
        return at(lax.rem(z + d + nz, nz), y, c, x)

    def segment(s):
        return at(s // (ny * nc), lax.rem(s // nc, ny), lax.rem(s, nc), x)

    def remote(src, dst, ssem, rsem, device):
        return pltpu.make_async_remote_copy(
            src_ref=src, dst_ref=dst, send_sem=ssem, recv_sem=rsem, device_id=device, device_id_type=MESH
        )

    def taken(ref, sem):
        pltpu.make_async_copy(ref, ref, sem).wait()

    barrier = pltpu.get_barrier_semaphore()

    def tell(device):
        pl.semaphore_signal(barrier, inc=1, device_id=device, device_id_type=MESH)

    for d in range(step, 0, -1):
        tell(zmate(-d))

        @pl.when(z + d < nz)
        def _(d=d):
            tell(zmate(d))

    up = jnp.logical_and(jnp.logical_and(y == ny - 1, c == nc - 1), z < nz - 1)
    down = jnp.logical_and(seat == 0, z > 0)

    @pl.when(up)
    def _():
        tell(segment(me + 1))

    @pl.when(down)
    def _():
        tell(segment(me - 1))

    for d in range(1, nx):
        tell(at(z, y, c, lax.rem(x + d, nx)))

    def tell_seat(j, carry):
        k = lax.rem(seat + j, seats)
        tell(at(z, k // nc, lax.rem(k, nc), x))
        return carry

    lax.fori_loop(1, seats, tell_seat, 0)
    peers = (
        step + jnp.minimum(z, step) + nx - 1 + seats - 1 + up.astype(jnp.int32) + down.astype(jnp.int32)
    )

    loads = [
        pltpu.make_async_copy(s, d, load_sem.at[i])
        for i, (s, d) in enumerate(
            (
                (k_hbm, kt_v), (v_hbm, vt_v), (q_hbm, q_v), (g_hbm, g_v), (o_hbm, o_v), (l_hbm, l_v), (ch_hbm, ch_v),
                (x_hbm, xg.at[x]),
            )
        )
    ]
    for cp in loads:
        cp.start()
    for cp in loads:
        cp.wait()

    tok = q_v.shape[0]
    nb = tok // BLOCK
    heads = q_v.shape[1] // DH
    width = heads * BLOCK
    kv_v[...] = jnp.concatenate([kt_v[...], vt_v[...]], axis=0).T
    low = lax.broadcasted_iota(jnp.int32, (BLOCK, 2 * DH), 1) < DH
    for b in range(nb):
        for hp in range(heads // 2):
            rows = pl.ds(b * BLOCK, BLOCK)
            cols = pl.ds(hp * 2 * DH, 2 * DH)
            qt = q_v[rows, cols].astype(F32) * (DH**-0.5)
            gt = g_v[rows, cols].astype(F32)
            qr = pltpu.roll(qt, DH, 1)
            gr = pltpu.roll(gt, DH, 1)
            for k, (qq, gg) in enumerate(((qt, gr), (qr, gt))):
                h = hp * 2 + k
                w_v[b, pl.ds(h * BLOCK, BLOCK), :] = jnp.where(low, qq, 0.0).astype(BF16)
                w_v[b, pl.ds((heads + h) * BLOCK, BLOCK), :] = jnp.where(low, 0.0, gg).astype(BF16)

    prod = g_v[...].astype(F32) * o_v[...].astype(F32)
    delta = jnp.sum(prod.T.reshape(heads, DH, tok), axis=1)
    lse = l_v[...] * LOG2E
    for b in range(nb):
        for h in range(heads):
            cols = pl.ds(h * BLOCK, BLOCK)
            drow[b, :, cols] = delta[h : h + 1, b * BLOCK : (b + 1) * BLOCK]
            lrow[b, :, cols] = lse[h : h + 1, b * BLOCK : (b + 1) * BLOCK]

    def tile(kv, b, l_of, keep):
        n = kv.shape[0] // BLOCK
        qw = w_v[b, pl.ds(0, width), :]
        gw = w_v[b, pl.ds(width, width), :]
        scores = nt(kv, qw)
        dprobs = nt(kv, gw)
        dl = drow[b]
        ps, ds = [], []
        for k in range(n):
            rows = slice(k * BLOCK, (k + 1) * BLOCK)
            p = jnp.exp2(scores[rows] * LOG2E - l_of(k))
            if keep is not None:
                p = jnp.where(keep, p, 0.0)
            ps.append(p.astype(BF16))
            ds.append((p * (dprobs[rows] - dl)).astype(BF16))
        p = ps[0] if n == 1 else jnp.concatenate(ps, axis=0)
        d = ds[0] if n == 1 else jnp.concatenate(ds, axis=0)
        dkv = nn(d, qw) + nn(p, gw)
        return dkv, tn(kv[:, :DH], d)

    keep = lax.broadcasted_iota(jnp.int32, (BLOCK, width), 0) <= lax.rem(
        lax.broadcasted_iota(jnp.int32, (BLOCK, width), 1), BLOCK
    )
    for b in range(nb):
        rows = pl.ds(b * BLOCK, BLOCK)
        dkv, dq = tile(kv_v[rows, :], b, lambda k: lrow[b], keep)
        dkv_own[rows, :] = dkv
        dqt[b] = dq

    pl.semaphore_wait(barrier, peers)

    reach = [1, total // 8, total // 4, total // 2]
    sends_to = [me + r < total for r in reach]
    gets_from = [me >= r for r in reach]
    kv_out = [remote(kv_v, far.at[l], kv_s.at[l], kv_r.at[l], segment(me + reach[l])) for l in range(3)]
    relayed = jnp.logical_and(z >= step, z + step < nz)
    kv_out.append(remote(far.at[2], far.at[3], kv_s.at[3], kv_r.at[3], zmate(step)))
    for l in (2, 1, 0):

        @pl.when(sends_to[l])
        def _(l=l):
            kv_out[l].start()

    def hello(sem, device):
        pl.semaphore_signal(sem, inc=1, device_id=device, device_id_type=MESH)

    hello(near_sem.at[0], zmate(step))

    @pl.when(z >= step)
    def _():
        hello(near_sem.at[0], zmate(-step))

    x_out = [
        remote(xg.at[x], xg.at[x], x_s.at[d - 1], x_r.at[x], at(z, y, c, lax.rem(x + d, nx))) for d in range(1, nx)
    ]

    @pl.when(x == 0)
    def _():
        for cp in x_out:
            cp.start()

    @pl.when(gets_from[2])
    def _():
        taken(far.at[2], kv_r.at[2])

    @pl.when(relayed)
    def _():
        kv_out[3].start()

    lane = lax.broadcasted_iota(jnp.int32, ch_v.shape, 1)

    def level(l):
        if l != 2:
            taken(far.at[l], kv_r.at[l])
        kv = far[l]
        acc = jnp.zeros((tok, 2 * DH), F32)
        for b in range(nb):
            own = jnp.where(lane == me * nb + b, ch_v[...].astype(F32), 0.0)
            sel = jnp.sum(own[PER * l : PER * (l + 1)], axis=1, keepdims=True)

            def l_of(k):
                want = ((me - reach[l]) * nb + k).astype(F32)
                hit = jnp.max(jnp.where(sel == want, 1.0, 0.0), axis=0, keepdims=True)
                return lrow[b] + (1.0 - hit) * BIG

            dkv, dq = tile(kv, b, l_of, None)
            dqt[b] = dqt[b] + dq
            acc = acc + dkv
        back[l] = acc.astype(BF16)

    ret_out = [remote(back.at[l], ret.at[l], r_s.at[l], r_r.at[l], segment(me - reach[l])) for l in range(LEVELS)]

    def run_level(l):
        @pl.when(gets_from[l])
        def _():
            level(l)

    def give_back(l):
        @pl.when(gets_from[l])
        def _():
            ret_out[l].start()

    def flip(b):
        for k in range(step):
            xt[b * step + k] = xg[b, :, pl.ds(k * 128, 128)].T

    def block_of_x(b):
        @pl.when(x != b)
        def _():
            taken(xg.at[b], x_r.at[b])

        flip(b)

    run_level(0)

    @pl.when(x != 0)
    def _():
        for cp in x_out:
            cp.start()

    run_level(1)
    give_back(0)
    run_level(2)
    give_back(1)
    block_of_x(0)
    give_back(2)
    pl.semaphore_wait(near_sem.at[0], 1 + (z + step < nz).astype(jnp.int32))
    hello(near_sem.at[1], zmate(-step))
    run_level(3)

    for b in range(nb):
        t = (dqt[b] * (DH**-0.5)).T
        for h in range(heads):
            dq_ref[pl.ds(b * BLOCK, BLOCK), pl.ds(h * DH, DH)] = t[h * BLOCK : (h + 1) * BLOCK].astype(BF16)
    dq = dq_ref[...]

    feats = 128

    def product(z0, n):
        return nn(xt[pl.ds(z0, n)].reshape(n * feats, tok), dq)

    def send_group(g):
        z0, n = groups[g]
        out = product(z0, n)
        for i in range(n):
            ys[g][:, i] = out[i * feats : (i + 1) * feats].reshape(seats, feats // seats, width).astype(BF16)
        yr[g][seat] = ys[g][seat]

        def to_seat(j, carry):
            k = lax.rem(seat + j, seats)
            remote(
                ys[g].at[k], yr[g].at[seat], y_s.at[g], y_r.at[g], at(z, k // nc, lax.rem(k, nc), x)
            ).start()
            return carry

        lax.fori_loop(1, seats, to_seat, 0)

    def to_owner(zz):
        @pl.when(zz != z)
        def _():
            remote(zs.at[zz], zr.at[z], z_s.at[zz], z_r.at[0], at(zz, y, c, x)).start()

        @pl.when(zz == z)
        def _():
            zr[z] = zs[zz]

    def sum_group(g):
        z0, n = groups[g]
        taken(yr[g].at[pl.ds(0, seats - 1)], y_r.at[g])
        acc = yr[g][0].astype(F32)
        for k in range(1, seats):
            acc = acc + yr[g][k].astype(F32)
        zs[pl.ds(z0, n)] = acc.astype(BF16)
        for i in range(n):
            to_owner(z0 + i)

    send_group(0)
    send_group(1)
    send_group(2)
    give_back(3)
    for b in range(1, half // step):
        block_of_x(b)
    for g in range(3, ng):
        send_group(g)
    pl.semaphore_wait(near_sem.at[1], 1)
    sum_group(0)
    sum_group(1)
    for b in range(half // step, nx):
        block_of_x(b)
    sum_group(2)

    def pair(i, carry):
        part = product(half + i, 1).reshape(ny, nc, feats // seats, width).astype(BF16)
        for e in range(nc):
            pe[e, :, i] = part[:, e]
        return carry

    lax.fori_loop(0, half, pair, 0)
    swap = remote(pe.at[1 - c], pr, p_s.at[0], p_r.at[0], at(z, y, 1 - c, x))
    swap.start()
    for g in range(3, ng):
        sum_group(g)
    swap.wait_recv()
    for yy in range(ny):
        ys2[yy] = (pe[c, yy].astype(F32) + pr[yy].astype(F32)).astype(BF16)
    yr2[y] = ys2[y]
    for d in range(1, ny):
        yy = lax.rem(y + d, ny)
        remote(ys2.at[yy], yr2.at[y], y2_s.at[0], y2_r.at[0], at(z, yy, c, x)).start()

    total_kv = dkv_own[...]
    for l in range(LEVELS):

        @pl.when(sends_to[l])
        def _(l=l):
            taken(ret.at[l], r_r.at[l])
            dkv_own[...] = dkv_own[...] + ret[l].astype(F32)

    total_kv = dkv_own[...].T
    dk_ref[...] = total_kv[:DH].astype(BF16)
    dv_ref[...] = total_kv[DH:].astype(BF16)

    taken(yr2.at[pl.ds(0, ny - 1)], y2_r.at[0])
    acc = yr2[0].astype(F32)
    for k in range(1, ny):
        acc = acc + yr2[k].astype(F32)
    zs[pl.ds(half, half)] = acc.astype(BF16)
    for i in range(half):
        to_owner(half + i)

    for l in range(LEVELS):

        @pl.when(sends_to[l] if l < 3 else relayed)
        def _(l=l):
            kv_out[l].wait_send()

        @pl.when(gets_from[l])
        def _(l=l):
            ret_out[l].wait_send()

    for cp in x_out:
        cp.wait_send()
    for g in range(ng):
        taken(ys[g].at[pl.ds(0, seats - 1)], y_s.at[g])
    swap.wait_send()
    taken(ys2.at[pl.ds(0, ny - 1)], y2_s.at[0])

    taken(zr.at[pl.ds(0, nz - 1)], z_r.at[0])
    acc = zr[0].astype(F32)
    for k in range(1, nz):
        acc = acc + zr[k].astype(F32)
    dw_ref[...] = acc

    def left(i, carry):
        @pl.when(i != z)
        def _():
            taken(zs.at[i], z_s.at[i])

        return carry

    lax.fori_loop(0, nz, left, 0)


def write(dq, dk, dv, dw, dq_out, dk_out, dv_out, dw_out, sem):
    copies = [
        pltpu.make_async_copy(s, d, sem.at[i])
        for i, (s, d) in enumerate(((dq, dq_out), (dk, dk_out), (dv, dv_out), (dw, dw_out)))
    ]
    for cp in copies:
        cp.start()
    for cp in copies:
        cp.wait()


def shards(layer_input, queries, keys, values, attn_out, grad_out, log_sum, chosen):
    nz, ny, nc, nx = (SIZES[a] for a in ("z", "y", "c", "x"))
    total = nz * ny * nc
    tok, qw = queries.shape
    nb = tok // BLOCK
    heads = qw // DH
    feats = layer_input.shape[1]
    rows_out = feats * nx // total
    half = nz // 2
    groups = groups_of(half)
    ng = len(groups)
    seats = ny * nc
    dma = pltpu.SemaphoreType.DMA
    vm = pltpu.VMEM
    hbm = pl.BlockSpec(memory_space=pltpu.HBM)
    vmem = pl.BlockSpec(memory_space=pltpu.VMEM)
    shapes = (
        jax.ShapeDtypeStruct((tok, qw), BF16),
        jax.ShapeDtypeStruct((DH, tok), BF16),
        jax.ShapeDtypeStruct((DH, tok), BF16),
        jax.ShapeDtypeStruct((rows_out, qw), F32),
    )
    parts = pl.pallas_call(
        kernel,
        out_shape=tuple(pltpu.VMEM(s.shape, s.dtype) for s in shapes),
        in_specs=[hbm] * 8,
        out_specs=(vmem,) * 4,
        scratch_shapes=[
            vm((tok, qw), BF16), vm((tok, qw), BF16), vm((tok, qw), BF16), vm((heads, tok), F32),
            vm((LEVELS * PER, chosen.shape[0]), jnp.int32), vm((DH, tok), BF16), vm((DH, tok), BF16), vm((tok, 2 * DH), BF16),
            vm((nb, 2 * heads * BLOCK, 2 * DH), BF16), vm((nb, 1, heads * BLOCK), F32), vm((nb, 1, heads * BLOCK), F32),
            vm((nb, DH, heads * BLOCK), F32), vm((tok, 2 * DH), F32),
            vm((LEVELS, tok, 2 * DH), BF16), vm((LEVELS, tok, 2 * DH), BF16), vm((LEVELS, tok, 2 * DH), BF16),
            vm((nx, tok, feats), BF16), vm((nz, feats * nx // nz, tok), BF16),
            *(vm((seats, n, rows_out, qw), BF16) for _, n in groups),
            *(vm((seats, n, rows_out, qw), BF16) for _, n in groups),
            vm((nc, ny, half, rows_out, qw), BF16), vm((ny, half, rows_out, qw), BF16),
            vm((ny, half, rows_out, qw), BF16), vm((ny, half, rows_out, qw), BF16),
            vm((nz, rows_out, qw), BF16), vm((nz, rows_out, qw), BF16),
            dma((8,)), dma((LEVELS,)), dma((LEVELS,)), dma((nx - 1,)), dma((nx,)), dma((LEVELS,)), dma((LEVELS,)),
            dma((ng,)), dma((ng,)), dma((1,)), dma((1,)), dma((1,)), dma((1,)), dma((nz,)), dma((1,)),
            pltpu.SemaphoreType.REGULAR((2,)),
        ],
        compiler_params=pltpu.CompilerParams(collective_id=0, has_side_effects=True, vmem_limit_bytes=48 * 1024 * 1024),
        name="whole",
    )(
        *(
            pltpu.with_memory_space_constraint(a, pltpu.HBM)
            for a in (layer_input, queries, keys.T, values.T, attn_out, grad_out, log_sum.T, chosen.T)
        )
    )
    parts = [pltpu.with_memory_space_constraint(a, pltpu.VMEM) for a in parts]
    dq, dk, dv, dw = pl.pallas_call(
        write,
        out_shape=shapes,
        in_specs=[vmem] * 4,
        out_specs=(hbm,) * 4,
        scratch_shapes=[dma((4,))],
        name="write",
    )(*parts)
    return dq, dk.T, dv.T, dw


def solution(mesh):
    torus = Mesh(
        mesh.devices.reshape(SIZES["z"], SIZES["y"], SIZES["c"], SIZES["x"]), ("z", "y", "c", "x")
    )
    spec = P(KV, "x")
    return jax.shard_map(
        shards,
        mesh=torus,
        in_specs=(spec,) * 7 + (P(),),
        out_specs=(spec,) * 4,
        check_vma=False,
    )
```

```python
import functools

import jax
import jax.numpy as jnp
from jax import lax
from jax.experimental import pallas as pl
from jax.experimental.pallas import tpu as pltpu
from jax.sharding import Mesh
from jax.sharding import PartitionSpec as P

MESH = pl.DeviceIdType.MESH
F32 = jnp.float32
BF16 = jnp.bfloat16

DH = 64
BLOCK = 64
PER = 2
LEVELS = 4
LOG2E = 1.4426950408889634
BIG = 1e30
SIZES = {"z": 16, "y": 8, "c": 2, "x": 4}
KV = ("z", "y", "c")


def nt(a, b):
    return lax.dot_general(a, b, (((1,), (1,)), ((), ())), preferred_element_type=F32)


def tn(a, b):
    return lax.dot_general(a, b, (((0,), (0,)), ((), ())), preferred_element_type=F32)


def nn(a, b):
    return lax.dot_general(a, b, (((1,), (0,)), ((), ())), preferred_element_type=F32)


def groups_of(end):
    cuts = [0, 1, 3, 5, end // 2, end]
    return [(a, b - a) for a, b in zip(cuts, cuts[1:])]


def kernel(
    x_hbm, q_hbm, k_hbm, v_hbm, o_hbm, g_hbm, l_hbm, ch_hbm,
    dq_ref, dk_ref, dv_ref, dw_ref,
    q_v, o_v, g_v, l_v, ch_v, kt_v, vt_v, kv_v,
    w_v, lrow, drow, dqt, dkv_own, far, park, back, ret,
    xg, xt, *rest,
):
    nz, ny, nc, nx = (SIZES[a] for a in ("z", "y", "c", "x"))
    groups = groups_of(nz)
    ng = len(groups)
    pe, pr, ys, yr = (rest[k * ng : (k + 1) * ng] for k in range(4))
    zs, zr, load_sem, kv_s, kv_r, x_s, x_r, r_s, r_r, p_s, p_r, y_s, y_r, z_s, z_r, near_sem = rest[4 * ng :]
    z, y, c, x = (lax.axis_index(a) for a in ("z", "y", "c", "x"))
    total = nz * ny * nc
    me = (z * ny + y) * nc + c
    seat = y * nc + c
    seats = ny * nc
    step = nz // 4

    def at(zz, yy, cc, xx):
        return {"z": zz, "y": yy, "c": cc, "x": xx}

    def zmate(d):
        return at(lax.rem(z + d + nz, nz), y, c, x)

    def segment(s):
        return at(s // (ny * nc), lax.rem(s // nc, ny), lax.rem(s, nc), x)

    def remote(src, dst, ssem, rsem, device):
        return pltpu.make_async_remote_copy(
            src_ref=src, dst_ref=dst, send_sem=ssem, recv_sem=rsem, device_id=device, device_id_type=MESH
        )

    def taken(ref, sem):
        pltpu.make_async_copy(ref, ref, sem).wait()

    barrier = pltpu.get_barrier_semaphore()

    def tell(device):
        pl.semaphore_signal(barrier, inc=1, device_id=device, device_id_type=MESH)

    for d in range(step, 0, -1):
        tell_down = zmate(-d)
        if d <= step // 2:
            tell(tell_down)
        else:

            @pl.when(jnp.logical_or(z < d, z - d >= nz // 2))
            def _(tell_down=tell_down):
                tell(tell_down)

        @pl.when(z + d < nz)
        def _(d=d):
            tell(zmate(d))

    up = jnp.logical_and(jnp.logical_and(y == ny - 1, c == nc - 1), z < nz - 1)
    down = jnp.logical_and(seat == 0, z > 0)

    @pl.when(up)
    def _():
        tell(segment(me + 1))

    @pl.when(down)
    def _():
        tell(segment(me - 1))

    for d in range(1, nx):
        tell(at(z, y, c, lax.rem(x + d, nx)))

    def tell_seat(j, carry):
        k = lax.rem(seat + j, seats)
        tell(at(z, k // nc, lax.rem(k, nc), x))
        return carry

    lax.fori_loop(1, seats, tell_seat, 0)
    above = jnp.where(z < nz // 2, step // 2, step)
    peers = (
        above + jnp.minimum(z, step) + nx - 1 + seats - 1 + up.astype(jnp.int32) + down.astype(jnp.int32)
    )

    loads = [
        pltpu.make_async_copy(s, d, load_sem.at[i])
        for i, (s, d) in enumerate(
            (
                (k_hbm, kt_v), (v_hbm, vt_v), (q_hbm, q_v), (g_hbm, g_v), (o_hbm, o_v), (l_hbm, l_v), (ch_hbm, ch_v),
                (x_hbm, xg.at[x]),
            )
        )
    ]
    for cp in loads:
        cp.start()
    for cp in loads:
        cp.wait()

    tok = q_v.shape[0]
    nb = tok // BLOCK
    heads = q_v.shape[1] // DH
    width = heads * BLOCK
    kv_v[...] = jnp.concatenate([kt_v[...], vt_v[...]], axis=0).T
    low = lax.broadcasted_iota(jnp.int32, (BLOCK, 2 * DH), 1) < DH
    for b in range(nb):
        for hp in range(heads // 2):
            rows = pl.ds(b * BLOCK, BLOCK)
            cols = pl.ds(hp * 2 * DH, 2 * DH)
            qt = q_v[rows, cols].astype(F32) * (DH**-0.5)
            gt = g_v[rows, cols].astype(F32)
            qr = pltpu.roll(qt, DH, 1)
            gr = pltpu.roll(gt, DH, 1)
            for k, (qq, gg) in enumerate(((qt, gr), (qr, gt))):
                h = hp * 2 + k
                w_v[b, pl.ds(h * BLOCK, BLOCK), :] = jnp.where(low, qq, 0.0).astype(BF16)
                w_v[b, pl.ds((heads + h) * BLOCK, BLOCK), :] = jnp.where(low, 0.0, gg).astype(BF16)

    prod = g_v[...].astype(F32) * o_v[...].astype(F32)
    delta = jnp.sum(prod.T.reshape(heads, DH, tok), axis=1)
    lse = l_v[...] * LOG2E
    for b in range(nb):
        for h in range(heads):
            cols = pl.ds(h * BLOCK, BLOCK)
            drow[b, :, cols] = delta[h : h + 1, b * BLOCK : (b + 1) * BLOCK]
            lrow[b, :, cols] = lse[h : h + 1, b * BLOCK : (b + 1) * BLOCK]

    def tile(kv, b, l_of, keep):
        n = kv.shape[0] // BLOCK
        qw = w_v[b, pl.ds(0, width), :]
        gw = w_v[b, pl.ds(width, width), :]
        scores = nt(kv, qw)
        dprobs = nt(kv, gw)
        dl = drow[b]
        ps, ds = [], []
        for k in range(n):
            rows = slice(k * BLOCK, (k + 1) * BLOCK)
            p = jnp.exp2(scores[rows] * LOG2E - l_of(k))
            if keep is not None:
                p = jnp.where(keep, p, 0.0)
            ps.append(p.astype(BF16))
            ds.append((p * (dprobs[rows] - dl)).astype(BF16))
        p = ps[0] if n == 1 else jnp.concatenate(ps, axis=0)
        d = ds[0] if n == 1 else jnp.concatenate(ds, axis=0)
        dkv = nn(d, qw) + nn(p, gw)
        return dkv, tn(kv[:, :DH], d)

    keep = lax.broadcasted_iota(jnp.int32, (BLOCK, width), 0) <= lax.rem(
        lax.broadcasted_iota(jnp.int32, (BLOCK, width), 1), BLOCK
    )
    for b in range(nb):
        rows = pl.ds(b * BLOCK, BLOCK)
        dkv, dq = tile(kv_v[rows, :], b, lambda k: lrow[b], keep)
        dkv_own[rows, :] = dkv
        dqt[b] = dq

    pl.semaphore_wait(barrier, peers)

    reach = [1, total // 8, total // 4, total // 2]
    sends_to = [me + r < total for r in reach]
    gets_from = [me >= r for r in reach]
    kv_out = [
        remote(kv_v, far.at[0], kv_s.at[0], kv_r.at[0], segment(me + reach[0])),
        remote(kv_v, far.at[1], kv_s.at[1], kv_r.at[1], zmate(step // 2)),
        remote(far.at[1], far.at[2], kv_s.at[2], kv_r.at[2], zmate(step // 2)),
        remote(far.at[2], far.at[3], kv_s.at[3], kv_r.at[3], zmate(step)),
        remote(kv_v, park, kv_s.at[4], kv_r.at[4], zmate(-step)),
        remote(park, far.at[3], kv_s.at[5], kv_r.at[3], zmate(-step)),
    ]
    goes = sends_to[:2] + [
        jnp.logical_and(z >= step // 2, z + step // 2 < nz),
        jnp.logical_and(z >= step, z < 2 * step),
        jnp.logical_and(z >= step, z < 2 * step),
        z < step,
    ]

    def pass_on(l):
        @pl.when(goes[l])
        def _():
            kv_out[l].start()

    pass_on(0)
    pass_on(1)
    pass_on(4)

    def hello(sem, device):
        pl.semaphore_signal(sem, inc=1, device_id=device, device_id_type=MESH)

    late = z >= nz // 2

    @pl.when(z >= step)
    def _():
        hello(near_sem.at[0], zmate(-step))

    @pl.when(late)
    def _():
        hello(near_sem.at[1], zmate(step))

    x_out = [
        remote(xg.at[x], xg.at[x], x_s.at[d - 1], x_r.at[x], at(z, y, c, lax.rem(x + d, nx))) for d in range(1, nx)
    ]

    for cp in x_out:
        cp.start()

    def arrived(l):
        @pl.when(gets_from[l])
        def _():
            taken(far.at[l], kv_r.at[l])

    arrived(1)
    pass_on(2)

    lane = lax.broadcasted_iota(jnp.int32, ch_v.shape, 1)

    def level(l):
        kv = far[l]
        acc = jnp.zeros((tok, 2 * DH), F32)
        for b in range(nb):
            own = jnp.where(lane == me * nb + b, ch_v[...].astype(F32), 0.0)
            sel = jnp.sum(own[PER * l : PER * (l + 1)], axis=1, keepdims=True)

            def l_of(k):
                want = ((me - reach[l]) * nb + k).astype(F32)
                hit = jnp.max(jnp.where(sel == want, 1.0, 0.0), axis=0, keepdims=True)
                return lrow[b] + (1.0 - hit) * BIG

            dkv, dq = tile(kv, b, l_of, None)
            dqt[b] = dqt[b] + dq
            acc = acc + dkv
        back[l] = acc.astype(BF16)

    ret_out = [remote(back.at[l], ret.at[l], r_s.at[l], r_r.at[l], segment(me - reach[l])) for l in range(LEVELS)]

    def run_level(l):
        @pl.when(gets_from[l])
        def _():
            level(l)

    def give_back(l):
        @pl.when(gets_from[l])
        def _():
            ret_out[l].start()

    def flip(b):
        for k in range(step):
            xt[b * step + k] = xg[b, :, pl.ds(k * 128, 128)].T

    def block_of_x(b):
        @pl.when(x != b)
        def _():
            taken(xg.at[b], x_r.at[b])

        flip(b)

    run_level(1)
    arrived(0)
    run_level(0)
    arrived(2)

    @pl.when(goes[3])
    def _():
        pl.semaphore_wait(near_sem.at[0], 1)
        kv_out[3].start()
        hello(near_sem.at[1], zmate(step))

    give_back(1)
    give_back(0)
    run_level(2)
    block_of_x(0)
    give_back(2)
    arrived(3)
    run_level(3)

    for b in range(nb):
        t = (dqt[b] * (DH**-0.5)).T
        for h in range(heads):
            dq_ref[pl.ds(b * BLOCK, BLOCK), pl.ds(h * DH, DH)] = t[h * BLOCK : (h + 1) * BLOCK].astype(BF16)
    dq = dq_ref[...]

    feats = 128

    def product(z0, n):
        return nn(xt[pl.ds(z0, n)].reshape(n * feats, tok), dq)

    swaps = [remote(pe[g].at[1 - c], pr[g], p_s.at[g], p_r.at[g], at(z, y, 1 - c, x)) for g in range(ng)]

    def pair(g):
        z0, n = groups[g]

        def one(i, carry):
            part = product(z0 + i, 1).reshape(ny, nc, feats // seats, width).astype(BF16)
            for e in range(nc):
                pe[g][e, :, i] = part[:, e]
            return carry

        lax.fori_loop(0, n, one, 0, unroll=n <= 2)
        swaps[g].start()

    def across_y(g):
        swaps[g].wait_recv()
        for yy in range(ny):
            ys[g][yy] = (pe[g][c, yy].astype(F32) + pr[g][yy].astype(F32)).astype(BF16)
        yr[g][y] = ys[g][y]
        for d in sorted(range(1, ny), key=lambda d: -min(d, ny - d)):
            yy = lax.rem(y + d, ny)
            remote(ys[g].at[yy], yr[g].at[y], y_s.at[g], y_r.at[g], at(z, yy, c, x)).start()

    def to_owner(zz):
        @pl.when(zz != z)
        def _():
            remote(zs.at[zz], zr.at[z], z_s.at[zz], z_r.at[0], at(zz, y, c, x)).start()

        @pl.when(zz == z)
        def _():
            zr[z] = zs[zz]

    def across_z(g):
        z0, n = groups[g]
        taken(yr[g].at[pl.ds(0, ny - 1)], y_r.at[g])
        acc = yr[g][0].astype(F32)
        for k in range(1, ny):
            acc = acc + yr[g][k].astype(F32)
        zs[pl.ds(z0, n)] = acc.astype(BF16)
        for i in range(n):
            to_owner(z0 + i)

    @pl.when(goes[5])
    def _():
        pl.semaphore_wait(near_sem.at[1], 1)
        taken(park, kv_r.at[4])
        kv_out[5].start()
        pl.semaphore_wait(near_sem.at[0], 1)
        hello(near_sem.at[1], zmate(step))

    pair(0)
    pair(1)
    give_back(3)
    block_of_x(1)
    across_y(0)
    pair(2)
    across_y(1)

    @pl.when(jnp.logical_and(late, z + step < nz))
    def _():
        pl.semaphore_wait(near_sem.at[0], 1)

    @pl.when(z >= step)
    def _():
        pl.semaphore_wait(near_sem.at[1], 1)

    hello(near_sem.at[2], zmate(-step))
    pair(3)
    across_y(2)
    across_y(3)
    block_of_x(2)
    block_of_x(3)
    pair(4)
    pl.semaphore_wait(near_sem.at[2], 1)
    across_z(0)
    across_z(1)
    across_y(4)
    across_z(2)
    across_z(3)

    for l in range(LEVELS):

        @pl.when(sends_to[l])
        def _(l=l):
            taken(ret.at[l], r_r.at[l])
            dkv_own[...] = dkv_own[...] + ret[l].astype(F32)

    total_kv = dkv_own[...].T
    dk_ref[...] = total_kv[:DH].astype(BF16)
    dv_ref[...] = total_kv[DH:].astype(BF16)
    across_z(4)

    for l in range(LEVELS + 2):

        @pl.when(goes[l])
        def _(l=l):
            kv_out[l].wait_send()

    for l in range(LEVELS):

        @pl.when(gets_from[l])
        def _(l=l):
            ret_out[l].wait_send()

    for cp in x_out:
        cp.wait_send()
    for g in range(ng):
        taken(ys[g].at[pl.ds(0, ny - 1)], y_s.at[g])
        swaps[g].wait_send()

    def left(i, carry):
        @pl.when(i != z)
        def _():
            taken(zs.at[i], z_s.at[i])

        return carry

    lax.fori_loop(0, nz, left, 0)

    taken(zr.at[pl.ds(0, nz - 1)], z_r.at[0])
    acc = zr[0].astype(F32)
    for k in range(1, nz):
        acc = acc + zr[k].astype(F32)
    dw_ref[...] = acc


def write(dq, dk, dv, dw, dq_out, dk_out, dv_out, dw_out, sem):
    copies = [
        pltpu.make_async_copy(s, d, sem.at[i])
        for i, (s, d) in enumerate(((dq, dq_out), (dk, dk_out), (dv, dv_out), (dw, dw_out)))
    ]
    for cp in copies:
        cp.start()
    for cp in copies:
        cp.wait()


def shards(layer_input, queries, keys, values, attn_out, grad_out, log_sum, chosen):
    nz, ny, nc, nx = (SIZES[a] for a in ("z", "y", "c", "x"))
    total = nz * ny * nc
    tok, qw = queries.shape
    nb = tok // BLOCK
    heads = qw // DH
    feats = layer_input.shape[1]
    rows_out = feats * nx // total
    groups = groups_of(nz)
    ng = len(groups)
    dma = pltpu.SemaphoreType.DMA
    vm = pltpu.VMEM
    hbm = pl.BlockSpec(memory_space=pltpu.HBM)
    vmem = pl.BlockSpec(memory_space=pltpu.VMEM)
    shapes = (
        jax.ShapeDtypeStruct((tok, qw), BF16),
        jax.ShapeDtypeStruct((DH, tok), BF16),
        jax.ShapeDtypeStruct((DH, tok), BF16),
        jax.ShapeDtypeStruct((rows_out, qw), F32),
    )
    parts = pl.pallas_call(
        kernel,
        out_shape=tuple(pltpu.VMEM(s.shape, s.dtype) for s in shapes),
        in_specs=[hbm] * 8,
        out_specs=(vmem,) * 4,
        scratch_shapes=[
            vm((tok, qw), BF16), vm((tok, qw), BF16), vm((tok, qw), BF16), vm((heads, tok), F32),
            vm((LEVELS * PER, chosen.shape[0]), jnp.int32), vm((DH, tok), BF16), vm((DH, tok), BF16), vm((tok, 2 * DH), BF16),
            vm((nb, 2 * heads * BLOCK, 2 * DH), BF16), vm((nb, 1, heads * BLOCK), F32), vm((nb, 1, heads * BLOCK), F32),
            vm((nb, DH, heads * BLOCK), F32), vm((tok, 2 * DH), F32),
            vm((LEVELS, tok, 2 * DH), BF16), vm((tok, 2 * DH), BF16), vm((LEVELS, tok, 2 * DH), BF16),
            vm((LEVELS, tok, 2 * DH), BF16),
            vm((nx, tok, feats), BF16), vm((nz, feats * nx // nz, tok), BF16),
            *(vm((nc, ny, n, rows_out, qw), BF16) for _, n in groups),
            *(vm((ny, n, rows_out, qw), BF16) for _ in range(3) for _, n in groups),
            vm((nz, rows_out, qw), BF16), vm((nz, rows_out, qw), BF16),
            dma((8,)), dma((LEVELS + 2,)), dma((LEVELS + 1,)), dma((nx - 1,)), dma((nx,)), dma((LEVELS,)), dma((LEVELS,)),
            dma((ng,)), dma((ng,)), dma((ng,)), dma((ng,)), dma((nz,)), dma((1,)),
            pltpu.SemaphoreType.REGULAR((3,)),
        ],
        compiler_params=pltpu.CompilerParams(collective_id=0, has_side_effects=True, vmem_limit_bytes=48 * 1024 * 1024),
        name="whole",
    )(
        *(
            pltpu.with_memory_space_constraint(a, pltpu.HBM)
            for a in (layer_input, queries, keys.T, values.T, attn_out, grad_out, log_sum.T, chosen.T)
        )
    )
    parts = [pltpu.with_memory_space_constraint(a, pltpu.VMEM) for a in parts]
    dq, dk, dv, dw = pl.pallas_call(
        write,
        out_shape=shapes,
        in_specs=[vmem] * 4,
        out_specs=(hbm,) * 4,
        scratch_shapes=[dma((4,))],
        name="write",
    )(*parts)
    return dq, dk.T, dv.T, dw


def solution(mesh):
    torus = Mesh(
        mesh.devices.reshape(SIZES["z"], SIZES["y"], SIZES["c"], SIZES["x"]), ("z", "y", "c", "x")
    )
    spec = P(KV, "x")
    return jax.shard_map(
        shards,
        mesh=torus,
        in_specs=(spec,) * 7 + (P(),),
        out_specs=(spec,) * 4,
        check_vma=False,
    )
```

```python
import functools

import jax
import jax.numpy as jnp
from jax import lax
from jax.experimental import pallas as pl
from jax.experimental.pallas import tpu as pltpu
from jax.sharding import Mesh
from jax.sharding import PartitionSpec as P

MESH = pl.DeviceIdType.MESH
F32 = jnp.float32
BF16 = jnp.bfloat16

DH = 64
BLOCK = 64
PER = 2
LEVELS = 4
LOG2E = 1.4426950408889634
BIG = 1e30
SIZES = {"z": 16, "y": 8, "c": 2, "x": 4}
KV = ("z", "y", "c")


def nt(a, b):
    return lax.dot_general(a, b, (((1,), (1,)), ((), ())), preferred_element_type=F32)


def tn(a, b):
    return lax.dot_general(a, b, (((0,), (0,)), ((), ())), preferred_element_type=F32)


def nn(a, b):
    return lax.dot_general(a, b, (((1,), (0,)), ((), ())), preferred_element_type=F32)


def groups_of(end):
    cuts = [0, 1, 3, 5, end // 2, end]
    return [(a, b - a) for a, b in zip(cuts, cuts[1:])]


def kernel(
    x_hbm, q_hbm, k_hbm, v_hbm, o_hbm, g_hbm, l_hbm, ch_hbm,
    dq_ref, dk_ref, dv_ref, dw_ref,
    qgo_v, l_v, ch_v, kvt_v, kv_v,
    w_v, lrow, nrow, drow, dqt, dkv_own, far, back, ret,
    xg, xt, *rest,
):
    nz, ny, nc, nx = (SIZES[a] for a in ("z", "y", "c", "x"))
    groups = groups_of(nz)
    ng = len(groups)
    pe, pr, ys, yr, zs, zr, sent, kv_r, x_r, r_r, p_r, y_r, z_r, near_sem = rest
    kv_s, x_s, r_s, p_s, y_s, z_s = (sent.at[i] for i in range(6))
    z, y, c, x = (lax.axis_index(a) for a in ("z", "y", "c", "x"))
    total = nz * ny * nc
    me = (z * ny + y) * nc + c
    seat = y * nc + c
    seats = ny * nc
    step = nz // 4

    def at(zz, yy, cc, xx):
        return {"z": zz, "y": yy, "c": cc, "x": xx}

    def zmate(d):
        return at(lax.rem(z + d + nz, nz), y, c, x)

    def segment(s):
        return at(s // (ny * nc), lax.rem(s // nc, ny), lax.rem(s, nc), x)

    def remote(src, dst, ssem, rsem, device):
        return pltpu.make_async_remote_copy(
            src_ref=src, dst_ref=dst, send_sem=ssem, recv_sem=rsem, device_id=device, device_id_type=MESH
        )

    def taken(ref, sem):
        pltpu.make_async_copy(ref, ref, sem).wait()

    barrier = pltpu.get_barrier_semaphore()

    def tell(device):
        pl.semaphore_signal(barrier, inc=1, device_id=device, device_id_type=MESH)

    late = z >= nz // 2
    last = nz - step
    for d in range(step, 0, -1):
        below, above = zmate(-d), zmate(d)
        if d <= step // 2:
            tell(below)
        else:

            @pl.when(z < d)
            def _(below=below):
                tell(below)

        @pl.when(z + d < nz if d <= step // 2 else jnp.logical_and(z + d < nz, jnp.logical_not(late)))
        def _(above=above):
            tell(above)

    beside = jnp.int32(0)
    for d in range(1, step + 1):
        near = d <= step // 2
        beside += jnp.where(jnp.logical_and(z >= d, jnp.logical_or(near, z - d < nz // 2)), 1, 0)
        beside += jnp.where(jnp.logical_or(z + d >= nz, near), 1, 0) * jnp.where(
            jnp.logical_or(z + d < nz, z >= last), 1, 0
        )

    up = jnp.logical_and(jnp.logical_and(y == ny - 1, c == nc - 1), z < nz - 1)
    down = jnp.logical_and(seat == 0, z > 0)

    @pl.when(up)
    def _():
        tell(segment(me + 1))

    @pl.when(down)
    def _():
        tell(segment(me - 1))

    for d in range(1, nx):
        tell(at(z, y, c, lax.rem(x + d, nx)))

    tell(at(z, y, 1 - c, x))
    for d in (2, 1):
        for e in range(nc):
            tell(at(z, lax.rem(y + d, ny), e, x))
            tell(at(z, lax.rem(y + ny - d, ny), e, x))
    peers = beside + nx - 1 + 1 + 4 * nc + up.astype(jnp.int32) + down.astype(jnp.int32)

    heads_at = ((k_hbm, kvt_v.at[0], kv_s), (v_hbm, kvt_v.at[1], kv_s), (q_hbm, qgo_v.at[0], x_s), (g_hbm, qgo_v.at[1], x_s))
    for src, dst, sem in (*heads_at, (o_hbm, qgo_v.at[2], x_s), (l_hbm, l_v, r_s), (ch_hbm, ch_v, p_s), (x_hbm, xg.at[x], y_s)):
        pltpu.make_async_copy(src, dst, sem).start()
    for ref, sem in ((kvt_v, kv_s), (qgo_v, x_s), (l_v, r_s), (ch_v, p_s), (xg.at[x], y_s)):
        taken(ref, sem)
    q_v, g_v, o_v = (qgo_v.at[i] for i in range(3))

    tok, heads = qgo_v.shape[1], qgo_v.shape[2] // DH
    nb = tok // BLOCK
    width = heads * BLOCK
    kv_v[...] = kvt_v[...].reshape(2 * DH, tok).T
    low = lax.broadcasted_iota(jnp.int32, (BLOCK, 2 * DH), 1) < DH
    for b in range(nb):
        for hp in range(heads // 2):
            rows = pl.ds(b * BLOCK, BLOCK)
            cols = pl.ds(hp * 2 * DH, 2 * DH)
            qt = q_v[rows, cols].astype(F32) * (DH**-0.5)
            gt = g_v[rows, cols].astype(F32)
            qr = pltpu.roll(qt, DH, 1)
            gr = pltpu.roll(gt, DH, 1)
            for k, (qq, gg) in enumerate(((qt, gr), (qr, gt))):
                h = hp * 2 + k
                w_v[b, pl.ds(h * BLOCK, BLOCK), :] = jnp.where(low, qq, 0.0).astype(BF16)
                w_v[b, pl.ds((heads + h) * BLOCK, BLOCK), :] = jnp.where(low, 0.0, gg).astype(BF16)

    prod = g_v[...].astype(F32) * o_v[...].astype(F32)
    delta = jnp.sum(prod.T.reshape(heads, DH, tok), axis=1)
    lse = l_v[...] * LOG2E
    for b in range(nb):
        for h in range(heads):
            cols = pl.ds(h * BLOCK, BLOCK)
            drow[b, :, cols] = delta[h : h + 1, b * BLOCK : (b + 1) * BLOCK]
            lrow[b, :, cols] = lse[h : h + 1, b * BLOCK : (b + 1) * BLOCK]

    reach = [1, total // 8, total // 4, total // 2]
    lane = lax.broadcasted_iota(jnp.int32, ch_v.shape, 1)
    for b in range(nb):
        sel = jnp.sum(jnp.where(lane == me * nb + b, ch_v[...].astype(F32), 0.0), axis=1, keepdims=True)
        for l in range(LEVELS):
            for k in range(nb):
                want = ((me - reach[l]) * nb + k).astype(F32)
                hit = jnp.max(jnp.where(sel[PER * l : PER * (l + 1)] == want, 1.0, 0.0), axis=0, keepdims=True)
                nrow[l, b, k] = lrow[b] + (1.0 - hit) * BIG

    def tile(kv, b, l_of, keep):
        n = kv.shape[0] // BLOCK
        qw = w_v[b, pl.ds(0, width), :]
        gw = w_v[b, pl.ds(width, width), :]
        scores = nt(kv, qw)
        dprobs = nt(kv, gw)
        dl = drow[b]
        ps, ds = [], []
        for k in range(n):
            rows = slice(k * BLOCK, (k + 1) * BLOCK)
            p = jnp.exp2(scores[rows] * LOG2E - l_of(k))
            if keep is not None:
                p = jnp.where(keep, p, 0.0)
            ps.append(p.astype(BF16))
            ds.append((p * (dprobs[rows] - dl)).astype(BF16))
        p = ps[0] if n == 1 else jnp.concatenate(ps, axis=0)
        d = ds[0] if n == 1 else jnp.concatenate(ds, axis=0)
        dkv = nn(jnp.concatenate([d, p], axis=1), w_v[b])
        return dkv, tn(kv[:, :DH], d)

    keep = lax.broadcasted_iota(jnp.int32, (BLOCK, width), 0) <= lax.rem(
        lax.broadcasted_iota(jnp.int32, (BLOCK, width), 1), BLOCK
    )
    for b in range(nb):
        rows = pl.ds(b * BLOCK, BLOCK)
        dkv, dq = tile(kv_v[rows, :], b, lambda k: lrow[b], keep)
        dkv_own[rows, :] = dkv
        dqt[b] = dq

    pl.semaphore_wait(barrier, peers)

    sends_to = [me + r < total for r in reach]
    gets_from = [me >= r for r in reach]
    kv_out = [
        remote(kv_v, far.at[0], kv_s, kv_r.at[0], segment(me + reach[0])),
        remote(kv_v, far.at[1], kv_s, kv_r.at[1], zmate(step // 2)),
        remote(far.at[1], far.at[2], kv_s, kv_r.at[2], zmate(step // 2)),
        remote(far.at[2], far.at[3], kv_s, kv_r.at[3], zmate(step)),
        remote(kv_v, far.at[4], kv_s, kv_r.at[3], zmate(-step)),
        remote(far.at[4], far.at[3], kv_s, kv_r.at[3], zmate(-step)),
    ]
    goes = sends_to[:2] + [
        jnp.logical_and(z >= step // 2, z + step // 2 < nz),
        jnp.logical_and(z >= step, z < 2 * step),
        jnp.logical_and(z >= step, z < 2 * step),
        z < step,
    ]

    def pass_on(l):
        @pl.when(goes[l])
        def _():
            kv_out[l].start()

    pass_on(0)
    pass_on(1)
    pass_on(4)

    def hello(sem, device):
        pl.semaphore_signal(sem, inc=1, device_id=device, device_id_type=MESH)

    @pl.when(jnp.logical_and(late, z < last))
    def _():
        hello(near_sem.at[0], zmate(-step))

    @pl.when(z >= last)
    def _():
        hello(near_sem.at[1], zmate(step))

    @pl.when(z == nz - 2)
    def _():
        hello(near_sem.at[2], zmate(-2))

    @pl.when(z == nz - 1)
    def _():
        hello(near_sem.at[2], zmate(1))

    for d in (2, -2):
        hello(near_sem.at[3], at(z, lax.rem(y + d + ny, ny), c, x))

    x_out = [
        remote(xg.at[x], xg.at[x], x_s, x_r.at[x], at(z, y, c, lax.rem(x + d, nx))) for d in range(1, nx)
    ]

    for cp in x_out:
        cp.start()

    def arrived(l):
        @pl.when(gets_from[l])
        def _():
            taken(far.at[l], kv_r.at[l])

    arrived(1)
    pass_on(2)

    def level(l):
        kv = far[l]
        acc = jnp.zeros((tok, 2 * DH), F32)
        for b in range(nb):
            dkv, dq = tile(kv, b, lambda k: nrow[l, b, k], None)
            dqt[b] = dqt[b] + dq
            acc = acc + dkv
        back[l] = acc.astype(BF16)

    ret_out = [remote(back.at[l], ret.at[l], r_s, r_r, segment(me - reach[l])) for l in range(LEVELS)]

    def run_level(l):
        @pl.when(gets_from[l])
        def _():
            level(l)

    def give_back(l):
        @pl.when(gets_from[l])
        def _():
            ret_out[l].start()

    def flip(b):
        for k in range(step):
            xt[b * step + k] = xg[b, :, pl.ds(k * 128, 128)].T

    def block_of_x(b):
        @pl.when(x != b)
        def _():
            taken(xg.at[b], x_r.at[b])

        flip(b)

    run_level(1)
    arrived(0)
    run_level(0)
    arrived(2)

    @pl.when(goes[3])
    def _():
        pl.semaphore_wait(near_sem.at[0], 1)
        kv_out[3].start()
        hello(near_sem.at[0], zmate(-step))

    give_back(1)
    give_back(0)
    run_level(2)
    give_back(2)

    arrived(3)
    run_level(3)

    @pl.when(goes[5])
    def _():
        pl.semaphore_wait(near_sem.at[1], 1)
        taken(far.at[4], kv_r.at[3])
        kv_out[5].start()

    block_of_x(0)

    for b in range(nb):
        t = (dqt[b] * (DH**-0.5)).T
        for h in range(heads):
            dq_ref[pl.ds(b * BLOCK, BLOCK), pl.ds(h * DH, DH)] = t[h * BLOCK : (h + 1) * BLOCK].astype(BF16)
    dq = dq_ref[...]

    feats = 128

    def product(z0, n):
        return nn(xt[pl.ds(z0, n)].reshape(n * feats, tok), dq)

    def rows_of(g):
        z0, n = groups[g]
        return pl.ds(z0, n)

    def pair(g):
        z0, n = groups[g]

        def one(i, carry):
            part = product(z0 + i, 1).reshape(ny, nc, feats // seats, width).astype(BF16)
            for e in range(nc):
                pe[e, z0 + i] = part[:, e]
            return carry

        lax.fori_loop(0, n, one, 0, unroll=n <= 2)
        rows = rows_of(g)
        remote(pe.at[1 - c, rows], pr.at[rows], p_s, p_r.at[g], at(z, y, 1 - c, x)).start()

    def across_y(g):
        rows = rows_of(g)
        taken(pr.at[rows], p_r.at[g])
        for yy in range(ny):
            ys[yy, rows] = (pe[c, rows, yy].astype(F32) + pr[rows, yy].astype(F32)).astype(BF16)
        yr[y, rows] = ys[y, rows]
        for d in sorted(range(1, ny), key=lambda d: -min(d, ny - d)):
            yy = lax.rem(y + d, ny)
            remote(ys.at[yy, rows], yr.at[y, rows], y_s, y_r.at[g], at(z, yy, c, x)).start()

    def to_owner(zz):
        @pl.when(zz != z)
        def _():
            remote(zs.at[zz], zr.at[z], z_s, z_r, at(zz, y, c, x)).start()

        @pl.when(zz == z)
        def _():
            zr[z] = zs[zz]

    def across_z(g):
        z0, n = groups[g]
        rows = rows_of(g)
        taken(yr.at[pl.ds(0, ny - 1), rows], y_r.at[g])
        acc = yr[0, rows].astype(F32)
        for k in range(1, ny):
            acc = acc + yr[k, rows].astype(F32)
        zs[rows] = acc.astype(BF16)
        for i in range(n):
            to_owner(z0 + i)

    @pl.when(jnp.logical_not(late))
    def _():
        pair(0)
        pair(1)
        pl.semaphore_wait(near_sem.at[3], 2)
        across_y(0)
        across_y(1)
        block_of_x(1)
        pair(2)
        across_y(2)
        block_of_x(2)
        block_of_x(3)
        pair(4)
        across_y(4)

        @pl.when(goes[5])
        def _():
            pl.semaphore_wait(near_sem.at[0], 1)

            @pl.when(z == 0)
            def _():
                pl.semaphore_wait(near_sem.at[2], 1)

            hello(near_sem.at[1], zmate(step))

        @pl.when(goes[3])
        def _():
            pl.semaphore_wait(near_sem.at[1], 1)
            hello(near_sem.at[1], zmate(step))

        pair(3)
        across_y(3)
        across_z(0)
        across_z(1)
        across_z(2)
        across_z(3)
        across_z(4)

    @pl.when(late)
    def _():
        pair(0)
        pair(1)
        pl.semaphore_wait(near_sem.at[3], 2)
        across_y(0)
        across_y(1)
        give_back(3)
        block_of_x(1)
        pair(2)
        pair(3)
        across_y(2)
        across_y(3)
        block_of_x(2)
        block_of_x(3)
        pair(4)

        @pl.when(z < last)
        def _():
            pl.semaphore_wait(near_sem.at[1], 1)

        @pl.when(z == last)
        def _():
            pl.semaphore_wait(near_sem.at[2], 1)

        across_z(0)
        across_z(1)
        across_y(4)
        across_z(2)
        across_z(3)

    def count(flags):
        return sum(f.astype(jnp.int32) for f in flags)

    def slots(ref, sem, number, most):
        for k in range(1, most + 1):

            @pl.when(number == k)
            def _(k=k):
                taken(ref.at[pl.ds(0, k)], sem)

    slots(ret, r_r, count(sends_to), LEVELS)
    for l in range(LEVELS):

        @pl.when(sends_to[l])
        def _(l=l):
            dkv_own[...] = dkv_own[...] + ret[l].astype(F32)

    total_kv = dkv_own[...].T
    dk_ref[...] = total_kv[:DH].astype(BF16)
    dv_ref[...] = total_kv[DH:].astype(BF16)

    @pl.when(late)
    def _():
        across_z(4)

    slots(far, kv_s, count(goes), LEVELS + 1)
    slots(back, r_s, count(gets_from), LEVELS)
    taken(xg.at[pl.ds(0, nx - 1)], x_s)
    taken(pr, p_s)
    taken(ys.at[pl.ds(0, ny - 1)], y_s)
    taken(zs.at[pl.ds(0, nz - 1)], z_s)
    taken(zr.at[pl.ds(0, nz - 1)], z_r)
    acc = zr[0].astype(F32)
    for k in range(1, nz):
        acc = acc + zr[k].astype(F32)
    dw_ref[...] = acc


def write(dq, dk, dv, dw, dq_out, dk_out, dv_out, dw_out, sem):
    copies = [
        pltpu.make_async_copy(s, d, sem.at[i])
        for i, (s, d) in enumerate(((dq, dq_out), (dk, dk_out), (dv, dv_out), (dw, dw_out)))
    ]
    for cp in copies:
        cp.start()
    for cp in copies:
        cp.wait()


def shards(layer_input, queries, keys, values, attn_out, grad_out, log_sum, chosen):
    nz, ny, nc, nx = (SIZES[a] for a in ("z", "y", "c", "x"))
    total = nz * ny * nc
    tok, qw = queries.shape
    nb = tok // BLOCK
    heads = qw // DH
    feats = layer_input.shape[1]
    rows_out = feats * nx // total
    groups = groups_of(nz)
    ng = len(groups)
    dma = pltpu.SemaphoreType.DMA
    vm = pltpu.VMEM
    hbm = pl.BlockSpec(memory_space=pltpu.HBM)
    vmem = pl.BlockSpec(memory_space=pltpu.VMEM)
    shapes = (
        jax.ShapeDtypeStruct((tok, qw), BF16),
        jax.ShapeDtypeStruct((DH, tok), BF16),
        jax.ShapeDtypeStruct((DH, tok), BF16),
        jax.ShapeDtypeStruct((rows_out, qw), F32),
    )
    parts = pl.pallas_call(
        kernel,
        out_shape=tuple(pltpu.VMEM(s.shape, s.dtype) for s in shapes),
        in_specs=[hbm] * 8,
        out_specs=(vmem,) * 4,
        scratch_shapes=[
            vm((3, tok, qw), BF16), vm((heads, tok), F32), vm((LEVELS * PER, chosen.shape[0]), jnp.int32),
            vm((2, DH, tok), BF16), vm((tok, 2 * DH), BF16),
            vm((nb, 2 * heads * BLOCK, 2 * DH), BF16), vm((nb, 1, heads * BLOCK), F32),
            vm((LEVELS, nb, nb, 1, heads * BLOCK), F32), vm((nb, 1, heads * BLOCK), F32),
            vm((nb, DH, heads * BLOCK), F32), vm((tok, 2 * DH), F32),
            vm((LEVELS + 1, tok, 2 * DH), BF16), vm((LEVELS, tok, 2 * DH), BF16), vm((LEVELS, tok, 2 * DH), BF16),
            vm((nx, tok, feats), BF16), vm((nz, feats * nx // nz, tok), BF16),
            vm((nc, nz, ny, rows_out, qw), BF16), vm((nz, ny, rows_out, qw), BF16),
            vm((ny, nz, rows_out, qw), BF16), vm((ny, nz, rows_out, qw), BF16),
            vm((nz, rows_out, qw), BF16), vm((nz, rows_out, qw), BF16),
            dma((6,)), dma((LEVELS,)), dma((nx,)), dma, dma((ng,)), dma((ng,)), dma,
            pltpu.SemaphoreType.REGULAR((4,)),
        ],
        compiler_params=pltpu.CompilerParams(collective_id=0, has_side_effects=True, vmem_limit_bytes=48 * 1024 * 1024),
        name="whole",
    )(
        *(
            pltpu.with_memory_space_constraint(a, pltpu.HBM)
            for a in (layer_input, queries, keys.T, values.T, attn_out, grad_out, log_sum.T, chosen.T)
        )
    )
    parts = [pltpu.with_memory_space_constraint(a, pltpu.VMEM) for a in parts]
    dq, dk, dv, dw = pl.pallas_call(
        write,
        out_shape=shapes,
        in_specs=[vmem] * 4,
        out_specs=(hbm,) * 4,
        scratch_shapes=[dma((4,))],
        name="write",
    )(*parts)
    return dq, dk.T, dv.T, dw


def solution(mesh):
    torus = Mesh(
        mesh.devices.reshape(SIZES["z"], SIZES["y"], SIZES["c"], SIZES["x"]), ("z", "y", "c", "x")
    )
    spec = P(KV, "x")
    return jax.shard_map(
        shards,
        mesh=torus,
        in_specs=(spec,) * 7 + (P(),),
        out_specs=(spec,) * 4,
        check_vma=False,
    )
```

```python
import functools

import jax
import jax.numpy as jnp
from jax import lax
from jax.experimental import pallas as pl
from jax.experimental.pallas import tpu as pltpu
from jax.sharding import Mesh
from jax.sharding import PartitionSpec as P

MESH = pl.DeviceIdType.MESH
F32 = jnp.float32
BF16 = jnp.bfloat16

DH = 64
BLOCK = 64
PER = 2
LEVELS = 4
LOG2E = 1.4426950408889634
BIG = 1e30
SIZES = {"z": 16, "y": 8, "c": 2, "x": 4}
KV = ("z", "y", "c")


def nt(a, b):
    return lax.dot_general(a, b, (((1,), (1,)), ((), ())), preferred_element_type=F32)


def tn(a, b):
    return lax.dot_general(a, b, (((0,), (0,)), ((), ())), preferred_element_type=F32)


def nn(a, b):
    return lax.dot_general(a, b, (((1,), (0,)), ((), ())), preferred_element_type=F32)


def groups_of(end):
    cuts = [0, 1, 3, 5, end // 2, end]
    return [(a, b - a) for a, b in zip(cuts, cuts[1:])]


def kernel(
    x_hbm, q_hbm, k_hbm, v_hbm, o_hbm, g_hbm, l_hbm, ch_hbm,
    dq_ref, dk_ref, dv_ref, dw_ref,
    qgo_v, l_v, ch_v, kvt_v, kv_v,
    w_v, dp_v, lrow, nrow, drow, dqt, dkv_own, far, back, ret,
    xg, xt, *rest,
):
    nz, ny, nc, nx = (SIZES[a] for a in ("z", "y", "c", "x"))
    groups = groups_of(nz)
    ng = len(groups)
    pe, pr, ys, yr, zs, zr, sent, kv_r, x_r, r_r, p_r, y_r, z_r, near_sem = rest
    kv_s, x_s, r_s, p_s, y_s, z_s = (sent.at[i] for i in range(6))
    z, y, c, x = (lax.axis_index(a) for a in ("z", "y", "c", "x"))
    total = nz * ny * nc
    me = (z * ny + y) * nc + c
    seat = y * nc + c
    seats = ny * nc
    step = nz // 4

    def at(zz, yy, cc, xx):
        return {"z": zz, "y": yy, "c": cc, "x": xx}

    def zmate(d):
        return at(lax.rem(z + d + nz, nz), y, c, x)

    def segment(s):
        return at(s // (ny * nc), lax.rem(s // nc, ny), lax.rem(s, nc), x)

    def remote(src, dst, ssem, rsem, device):
        return pltpu.make_async_remote_copy(
            src_ref=src, dst_ref=dst, send_sem=ssem, recv_sem=rsem, device_id=device, device_id_type=MESH
        )

    def taken(ref, sem):
        pltpu.make_async_copy(ref, ref, sem).wait()

    barrier = pltpu.get_barrier_semaphore()

    def tell(device):
        pl.semaphore_signal(barrier, inc=1, device_id=device, device_id_type=MESH)

    late = z >= nz // 2
    last = nz - step
    for d in range(step, 0, -1):
        below, above = zmate(-d), zmate(d)
        if d <= step // 2:
            tell(below)
        else:

            @pl.when(z < d)
            def _(below=below):
                tell(below)

        @pl.when(z + d < nz if d <= step // 2 else jnp.logical_and(z + d < nz, jnp.logical_not(late)))
        def _(above=above):
            tell(above)

    beside = jnp.int32(0)
    for d in range(1, step + 1):
        near = d <= step // 2
        beside += jnp.where(jnp.logical_and(z >= d, jnp.logical_or(near, z - d < nz // 2)), 1, 0)
        beside += jnp.where(jnp.logical_or(z + d >= nz, near), 1, 0) * jnp.where(
            jnp.logical_or(z + d < nz, z >= last), 1, 0
        )

    up = jnp.logical_and(jnp.logical_and(y == ny - 1, c == nc - 1), z < nz - 1)
    down = jnp.logical_and(seat == 0, z > 0)

    @pl.when(up)
    def _():
        tell(segment(me + 1))

    @pl.when(down)
    def _():
        tell(segment(me - 1))

    for d in range(1, nx):
        tell(at(z, y, c, lax.rem(x + d, nx)))

    tell(at(z, y, 1 - c, x))
    for d in (2, 1):
        for e in range(nc):
            tell(at(z, lax.rem(y + d, ny), e, x))
            tell(at(z, lax.rem(y + ny - d, ny), e, x))
    peers = beside + nx - 1 + 1 + 4 * nc + up.astype(jnp.int32) + down.astype(jnp.int32)

    heads_at = ((k_hbm, kvt_v.at[0], kv_s), (v_hbm, kvt_v.at[1], kv_s), (q_hbm, qgo_v.at[0], x_s), (g_hbm, qgo_v.at[1], x_s))
    for src, dst, sem in (*heads_at, (o_hbm, qgo_v.at[2], x_s), (l_hbm, l_v, r_s), (ch_hbm, ch_v, p_s), (x_hbm, xg.at[x], y_s)):
        pltpu.make_async_copy(src, dst, sem).start()
    taken(kvt_v, kv_s)
    tok, heads = qgo_v.shape[1], qgo_v.shape[2] // DH
    nb = tok // BLOCK
    width = heads * BLOCK
    reach = [1, total // 8, total // 4, total // 2]
    kv_v[...] = kvt_v[...].reshape(2 * DH, tok).T
    pl.semaphore_wait(barrier, peers)

    sends_to = [me + r < total for r in reach]
    gets_from = [me >= r for r in reach]
    kv_out = [
        remote(kv_v, far.at[0], kv_s, kv_r.at[0], segment(me + reach[0])),
        remote(kv_v, far.at[1], kv_s, kv_r.at[1], zmate(step // 2)),
        remote(far.at[1], far.at[2], kv_s, kv_r.at[2], zmate(step // 2)),
        remote(far.at[2], far.at[3], kv_s, kv_r.at[3], zmate(step)),
        remote(kv_v, far.at[4], kv_s, kv_r.at[3], zmate(-step)),
        remote(far.at[4], far.at[3], kv_s, kv_r.at[3], zmate(-step)),
    ]
    goes = sends_to[:2] + [
        jnp.logical_and(z >= step // 2, z + step // 2 < nz),
        jnp.logical_and(z >= step, z < 2 * step),
        jnp.logical_and(z >= step, z < 2 * step),
        z < step,
    ]

    def pass_on(l):
        @pl.when(goes[l])
        def _():
            kv_out[l].start()

    pass_on(0)
    pass_on(1)
    pass_on(4)

    def hello(sem, device):
        pl.semaphore_signal(sem, inc=1, device_id=device, device_id_type=MESH)

    @pl.when(jnp.logical_and(late, z < last))
    def _():
        hello(near_sem.at[0], zmate(-step))

    @pl.when(z >= last)
    def _():
        hello(near_sem.at[1], zmate(step))

    @pl.when(z == nz - 2)
    def _():
        hello(near_sem.at[2], zmate(-2))

    @pl.when(z == nz - 1)
    def _():
        hello(near_sem.at[2], zmate(1))

    for d in (2, -2):
        hello(near_sem.at[3], at(z, lax.rem(y + d + ny, ny), c, x))

    x_out = [
        remote(xg.at[x], xg.at[x], x_s, x_r.at[x], at(z, y, c, lax.rem(x + d, nx))) for d in range(1, nx)
    ]

    taken(qgo_v, x_s)
    taken(xg.at[x], y_s)
    for cp in x_out:
        cp.start()

    taken(l_v, r_s)
    taken(ch_v, p_s)
    q_v, g_v, o_v = (qgo_v.at[i] for i in range(3))

    low = lax.broadcasted_iota(jnp.int32, (BLOCK, 2 * DH), 1) < DH
    for b in range(nb):
        for hp in range(heads // 2):
            rows = pl.ds(b * BLOCK, BLOCK)
            cols = pl.ds(hp * 2 * DH, 2 * DH)
            qt = q_v[rows, cols].astype(F32) * (DH**-0.5)
            gt = g_v[rows, cols].astype(F32)
            qr = pltpu.roll(qt, DH, 1)
            gr = pltpu.roll(gt, DH, 1)
            for k, (qq, gg) in enumerate(((qt, gr), (qr, gt))):
                h = hp * 2 + k
                w_v[b, pl.ds(h * BLOCK, BLOCK), :] = jnp.where(low, qq, 0.0).astype(BF16)
                w_v[b, pl.ds((heads + h) * BLOCK, BLOCK), :] = jnp.where(low, 0.0, gg).astype(BF16)

    prod = g_v[...].astype(F32) * o_v[...].astype(F32)
    delta = jnp.sum(prod.T.reshape(heads, DH, tok), axis=1)
    lse = l_v[...] * LOG2E
    for b in range(nb):
        for h in range(heads):
            cols = pl.ds(h * BLOCK, BLOCK)
            drow[b, :, cols] = delta[h : h + 1, b * BLOCK : (b + 1) * BLOCK]
            lrow[b, :, cols] = lse[h : h + 1, b * BLOCK : (b + 1) * BLOCK]

    lane = lax.broadcasted_iota(jnp.int32, ch_v.shape, 1)
    for b in range(nb):
        sel = jnp.sum(jnp.where(lane == me * nb + b, ch_v[...].astype(F32), 0.0), axis=1, keepdims=True)
        for l in range(LEVELS):
            for k in range(nb):
                want = ((me - reach[l]) * nb + k).astype(F32)
                hit = jnp.max(jnp.where(sel[PER * l : PER * (l + 1)] == want, 1.0, 0.0), axis=0, keepdims=True)
                nrow[l, b, k] = lrow[b] + (1.0 - hit) * BIG

    def first(kv, b):
        return nt(kv, w_v[b, pl.ds(0, width), :]), nt(kv, w_v[b, pl.ds(width, width), :])

    def middle(scores, dprobs, b, l_of, keep):
        dl = drow[b]
        ps, ds = [], []
        for k in range(scores.shape[0] // BLOCK):
            rows = slice(k * BLOCK, (k + 1) * BLOCK)
            p = jnp.exp2(scores[rows] * LOG2E - l_of(k))
            if keep is not None:
                p = jnp.where(keep, p, 0.0)
            ps.append(p.astype(BF16))
            ds.append((p * (dprobs[rows] - dl)).astype(BF16))
        return jnp.concatenate([jnp.concatenate(ds, axis=0), jnp.concatenate(ps, axis=0)], axis=1)

    def second(kv, b, dp):
        return nn(dp, w_v[b]), tn(kv[:, :DH], dp[:, :width])

    def tile(kv, b, l_of, keep):
        return second(kv, b, middle(*first(kv, b), b, l_of, keep))

    keep = lax.broadcasted_iota(jnp.int32, (BLOCK, width), 0) <= lax.rem(
        lax.broadcasted_iota(jnp.int32, (BLOCK, width), 1), BLOCK
    )
    for b in range(nb):
        rows = pl.ds(b * BLOCK, BLOCK)
        dkv, dq = tile(kv_v[rows, :], b, lambda k: lrow[b], keep)
        dkv_own[rows, :] = dkv
        dqt[b] = dq

    def arrived(l):
        @pl.when(gets_from[l])
        def _():
            taken(far.at[l], kv_r.at[l])

    arrived(1)
    pass_on(2)

    def terms(l):
        kv = far[l]
        raw = [first(kv, b) for b in range(nb)]
        dps = [middle(*raw[b], b, lambda k, b=b: nrow[l, b, k], None) for b in range(nb)]
        for b in range(nb):
            dqt[b] = dqt[b] + tn(kv[:, :DH], dps[b][:, :width])
        return jnp.concatenate(dps, axis=1)

    def toward_keys(l, dps):
        back[l] = nn(dps, w_v[...].reshape(nb * 2 * width, 2 * DH)).astype(BF16)

    def level(l):
        toward_keys(l, terms(l))

    ret_out = [remote(back.at[l], ret.at[l], r_s, r_r, segment(me - reach[l])) for l in range(LEVELS)]

    def run_level(l):
        @pl.when(gets_from[l])
        def _():
            level(l)

    def give_back(l):
        @pl.when(gets_from[l])
        def _():
            ret_out[l].start()

    def flip(b):
        for k in range(step):
            xt[b * step + k] = xg[b, :, pl.ds(k * 128, 128)].T

    def block_of_x(b):
        @pl.when(x != b)
        def _():
            taken(xg.at[b], x_r.at[b])

        flip(b)

    run_level(1)
    arrived(0)
    run_level(0)
    arrived(2)

    @pl.when(goes[3])
    def _():
        pl.semaphore_wait(near_sem.at[0], 1)
        kv_out[3].start()
        hello(near_sem.at[0], zmate(-step))

    give_back(1)
    give_back(0)
    run_level(2)
    give_back(2)

    arrived(3)

    @pl.when(late)
    def _():
        dp_v[...] = terms(3)

    @pl.when(goes[5])
    def _():
        pl.semaphore_wait(near_sem.at[1], 1)
        taken(far.at[4], kv_r.at[3])
        kv_out[5].start()

    block_of_x(0)

    for b in range(nb):
        t = (dqt[b] * (DH**-0.5)).astype(BF16).T
        for h in range(heads):
            dq_ref[pl.ds(b * BLOCK, BLOCK), pl.ds(h * DH, DH)] = t[h * BLOCK : (h + 1) * BLOCK]
    dq = dq_ref[...]

    feats = 128

    def product(z0, n):
        return nn(xt[pl.ds(z0, n)].reshape(n * feats, tok), dq)

    def rows_of(g):
        z0, n = groups[g]
        return pl.ds(z0, n)

    def pair(g):
        z0, n = groups[g]

        def one(i, carry):
            part = product(z0 + i, 1).reshape(ny, nc, feats // seats, width).astype(BF16)
            for e in range(nc):
                pe[e, z0 + i] = part[:, e]
            return carry

        lax.fori_loop(0, n, one, 0, unroll=n <= 2)
        rows = rows_of(g)
        remote(pe.at[1 - c, rows], pr.at[rows], p_s, p_r.at[g], at(z, y, 1 - c, x)).start()

    def across_y(g):
        rows = rows_of(g)
        taken(pr.at[rows], p_r.at[g])
        for yy in range(ny):
            ys[yy, rows] = (pe[c, rows, yy].astype(F32) + pr[rows, yy].astype(F32)).astype(BF16)
        yr[y, rows] = ys[y, rows]
        for d in sorted(range(1, ny), key=lambda d: -min(d, ny - d)):
            yy = lax.rem(y + d, ny)
            remote(ys.at[yy, rows], yr.at[y, rows], y_s, y_r.at[g], at(z, yy, c, x)).start()

    def to_owner(zz):
        @pl.when(zz != z)
        def _():
            remote(zs.at[zz], zr.at[z], z_s, z_r, at(zz, y, c, x)).start()

        @pl.when(zz == z)
        def _():
            zr[z] = zs[zz]

    def across_z(g):
        z0, n = groups[g]
        rows = rows_of(g)
        taken(yr.at[pl.ds(0, ny - 1), rows], y_r.at[g])
        acc = yr[0, rows].astype(F32)
        for k in range(1, ny):
            acc = acc + yr[k, rows].astype(F32)
        zs[rows] = acc.astype(BF16)
        for i in range(n):
            to_owner(z0 + i)

    @pl.when(jnp.logical_not(late))
    def _():
        pair(0)
        pair(1)
        pl.semaphore_wait(near_sem.at[3], 2)
        across_y(0)
        across_y(1)
        block_of_x(1)
        pair(2)
        across_y(2)
        block_of_x(2)
        block_of_x(3)
        pair(4)
        across_y(4)

        @pl.when(goes[5])
        def _():
            pl.semaphore_wait(near_sem.at[0], 1)

            @pl.when(z == 0)
            def _():
                pl.semaphore_wait(near_sem.at[2], 1)

            hello(near_sem.at[1], zmate(step))

        @pl.when(goes[3])
        def _():
            pl.semaphore_wait(near_sem.at[1], 1)
            hello(near_sem.at[1], zmate(step))

        pair(3)
        across_y(3)
        across_z(0)
        across_z(1)
        across_z(2)
        across_z(3)
        across_z(4)

    @pl.when(late)
    def _():
        pair(0)
        pair(1)
        pl.semaphore_wait(near_sem.at[3], 2)
        across_y(0)
        across_y(1)
        toward_keys(3, dp_v[...])
        ret_out[3].start()
        block_of_x(1)
        pair(2)
        pair(3)
        across_y(2)
        across_y(3)
        block_of_x(2)
        block_of_x(3)
        pair(4)

        @pl.when(z < last)
        def _():
            pl.semaphore_wait(near_sem.at[1], 1)

        @pl.when(z == last)
        def _():
            pl.semaphore_wait(near_sem.at[2], 1)

        across_z(0)
        across_z(1)
        across_y(4)
        across_z(2)
        across_z(3)

    def count(flags):
        return sum(f.astype(jnp.int32) for f in flags)

    def slots(ref, sem, number, most):
        for k in range(1, most + 1):

            @pl.when(number == k)
            def _(k=k):
                taken(ref.at[pl.ds(0, k)], sem)

    slots(ret, r_r, count(sends_to), LEVELS)
    for l in range(LEVELS):

        @pl.when(sends_to[l])
        def _(l=l):
            dkv_own[...] = dkv_own[...] + ret[l].astype(F32)

    total_kv = dkv_own[...].T
    dk_ref[...] = total_kv[:DH].astype(BF16)
    dv_ref[...] = total_kv[DH:].astype(BF16)

    @pl.when(late)
    def _():
        across_z(4)

    slots(far, kv_s, count(goes), LEVELS + 1)
    slots(back, r_s, count(gets_from), LEVELS)
    taken(xg.at[pl.ds(0, nx - 1)], x_s)
    taken(pr, p_s)
    taken(ys.at[pl.ds(0, ny - 1)], y_s)
    taken(zs.at[pl.ds(0, nz - 1)], z_s)
    taken(zr.at[pl.ds(0, nz - 1)], z_r)
    acc = zr[0].astype(F32)
    for k in range(1, nz):
        acc = acc + zr[k].astype(F32)
    dw_ref[...] = acc


def write(dq, dk, dv, dw, dq_out, dk_out, dv_out, dw_out, sem):
    copies = [
        pltpu.make_async_copy(s, d, sem.at[i])
        for i, (s, d) in enumerate(((dq, dq_out), (dk, dk_out), (dv, dv_out), (dw, dw_out)))
    ]
    for cp in copies:
        cp.start()
    for cp in copies:
        cp.wait()


def shards(layer_input, queries, keys, values, attn_out, grad_out, log_sum, chosen):
    nz, ny, nc, nx = (SIZES[a] for a in ("z", "y", "c", "x"))
    total = nz * ny * nc
    tok, qw = queries.shape
    nb = tok // BLOCK
    heads = qw // DH
    feats = layer_input.shape[1]
    rows_out = feats * nx // total
    groups = groups_of(nz)
    ng = len(groups)
    dma = pltpu.SemaphoreType.DMA
    vm = pltpu.VMEM
    hbm = pl.BlockSpec(memory_space=pltpu.HBM)
    vmem = pl.BlockSpec(memory_space=pltpu.VMEM)
    shapes = (
        jax.ShapeDtypeStruct((tok, qw), BF16),
        jax.ShapeDtypeStruct((DH, tok), BF16),
        jax.ShapeDtypeStruct((DH, tok), BF16),
        jax.ShapeDtypeStruct((rows_out, qw), F32),
    )
    parts = pl.pallas_call(
        kernel,
        out_shape=tuple(pltpu.VMEM(s.shape, s.dtype) for s in shapes),
        in_specs=[hbm] * 8,
        out_specs=(vmem,) * 4,
        scratch_shapes=[
            vm((3, tok, qw), BF16), vm((heads, tok), F32), vm((LEVELS * PER, chosen.shape[0]), jnp.int32),
            vm((2, DH, tok), BF16), vm((tok, 2 * DH), BF16),
            vm((nb, 2 * heads * BLOCK, 2 * DH), BF16), vm((tok, nb * 2 * heads * BLOCK), BF16),
            vm((nb, 1, heads * BLOCK), F32),
            vm((LEVELS, nb, nb, 1, heads * BLOCK), F32), vm((nb, 1, heads * BLOCK), F32),
            vm((nb, DH, heads * BLOCK), F32), vm((tok, 2 * DH), F32),
            vm((LEVELS + 1, tok, 2 * DH), BF16), vm((LEVELS, tok, 2 * DH), BF16), vm((LEVELS, tok, 2 * DH), BF16),
            vm((nx, tok, feats), BF16), vm((nz, feats * nx // nz, tok), BF16),
            vm((nc, nz, ny, rows_out, qw), BF16), vm((nz, ny, rows_out, qw), BF16),
            vm((ny, nz, rows_out, qw), BF16), vm((ny, nz, rows_out, qw), BF16),
            vm((nz, rows_out, qw), BF16), vm((nz, rows_out, qw), BF16),
            dma((6,)), dma((LEVELS,)), dma((nx,)), dma, dma((ng,)), dma((ng,)), dma,
            pltpu.SemaphoreType.REGULAR((4,)),
        ],
        compiler_params=pltpu.CompilerParams(collective_id=0, has_side_effects=True, vmem_limit_bytes=48 * 1024 * 1024),
        name="whole",
    )(
        *(
            pltpu.with_memory_space_constraint(a, pltpu.HBM)
            for a in (layer_input, queries, keys.T, values.T, attn_out, grad_out, log_sum.T, chosen.T)
        )
    )
    parts = [pltpu.with_memory_space_constraint(a, pltpu.VMEM) for a in parts]
    dq, dk, dv, dw = pl.pallas_call(
        write,
        out_shape=shapes,
        in_specs=[vmem] * 4,
        out_specs=(hbm,) * 4,
        scratch_shapes=[dma((4,))],
        name="write",
    )(*parts)
    return dq, dk.T, dv.T, dw


def solution(mesh):
    torus = Mesh(
        mesh.devices.reshape(SIZES["z"], SIZES["y"], SIZES["c"], SIZES["x"]), ("z", "y", "c", "x")
    )
    spec = P(KV, "x")
    return jax.shard_map(
        shards,
        mesh=torus,
        in_specs=(spec,) * 7 + (P(),),
        out_specs=(spec,) * 4,
        check_vma=False,
    )
```

```python
import functools

import jax
import jax.numpy as jnp
from jax import lax
from jax.experimental import pallas as pl
from jax.experimental.pallas import tpu as pltpu
from jax.sharding import Mesh
from jax.sharding import PartitionSpec as P

MESH = pl.DeviceIdType.MESH
F32 = jnp.float32
BF16 = jnp.bfloat16

DH = 64
BLOCK = 64
PER = 2
LEVELS = 4
LOG2E = 1.4426950408889634
BIG = 1e30
SIZES = {"z": 16, "y": 8, "c": 2, "x": 4}
KV = ("z", "y", "c")


def nt(a, b):
    return lax.dot_general(a, b, (((1,), (1,)), ((), ())), preferred_element_type=F32)


def tn(a, b):
    return lax.dot_general(a, b, (((0,), (0,)), ((), ())), preferred_element_type=F32)


def nn(a, b):
    return lax.dot_general(a, b, (((1,), (0,)), ((), ())), preferred_element_type=F32)


def groups_of(end):
    cuts = [0, 2, 4, end // 2, end]
    return [(a, b - a) for a, b in zip(cuts, cuts[1:])]


def kernel(
    x_hbm, q_hbm, k_hbm, v_hbm, o_hbm, g_hbm, l_hbm, ch_hbm,
    dq_ref, dk_ref, dv_ref, dw_ref,
    qgo_v, l_v, ch_v, kvt_v, kv_v,
    w_v, dp_v, lrow, nrow, drow, dqt, dkv_own, far, back, ret,
    xg, xt, *rest,
):
    nz, ny, nc, nx = (SIZES[a] for a in ("z", "y", "c", "x"))
    groups = groups_of(nz)
    ng = len(groups)
    pe, pr, ys, yr, zs, zr, sent, kv_r, x_r, r_r, p_r, y_r, z_r, near_sem = rest
    kv_s, x_s, r_s, p_s, y_s, z_s = (sent.at[i] for i in range(6))
    z, y, c, x = (lax.axis_index(a) for a in ("z", "y", "c", "x"))
    total = nz * ny * nc
    me = (z * ny + y) * nc + c
    seat = y * nc + c
    seats = ny * nc
    step = nz // 4

    def at(zz, yy, cc, xx):
        return {"z": zz, "y": yy, "c": cc, "x": xx}

    def zmate(d):
        return at(lax.rem(z + d + nz, nz), y, c, x)

    def segment(s):
        return at(s // (ny * nc), lax.rem(s // nc, ny), lax.rem(s, nc), x)

    def remote(src, dst, ssem, rsem, device):
        return pltpu.make_async_remote_copy(
            src_ref=src, dst_ref=dst, send_sem=ssem, recv_sem=rsem, device_id=device, device_id_type=MESH
        )

    def taken(ref, sem):
        pltpu.make_async_copy(ref, ref, sem).wait()

    barrier = pltpu.get_barrier_semaphore()

    def tell(device):
        pl.semaphore_signal(barrier, inc=1, device_id=device, device_id_type=MESH)

    late = z >= nz // 2
    last = nz - step
    for d in range(step, 0, -1):
        below, above = zmate(-d), zmate(d)
        if d <= step // 2:
            tell(below)
        else:

            @pl.when(z < d)
            def _(below=below):
                tell(below)

        @pl.when(z + d < nz if d <= step // 2 else jnp.logical_and(z + d < nz, jnp.logical_not(late)))
        def _(above=above):
            tell(above)

    beside = jnp.int32(0)
    for d in range(1, step + 1):
        near = d <= step // 2
        beside += jnp.where(jnp.logical_and(z >= d, jnp.logical_or(near, z - d < nz // 2)), 1, 0)
        beside += jnp.where(jnp.logical_or(z + d >= nz, near), 1, 0) * jnp.where(
            jnp.logical_or(z + d < nz, z >= last), 1, 0
        )

    up = jnp.logical_and(jnp.logical_and(y == ny - 1, c == nc - 1), z < nz - 1)
    down = jnp.logical_and(seat == 0, z > 0)

    @pl.when(up)
    def _():
        tell(segment(me + 1))

    @pl.when(down)
    def _():
        tell(segment(me - 1))

    for d in range(1, nx):
        tell(at(z, y, c, lax.rem(x + d, nx)))

    tell(at(z, y, 1 - c, x))
    for d in (2, 1):
        for e in range(nc):
            tell(at(z, lax.rem(y + d, ny), e, x))
            tell(at(z, lax.rem(y + ny - d, ny), e, x))
    peers = beside + nx - 1 + 1 + 4 * nc + up.astype(jnp.int32) + down.astype(jnp.int32)

    heads_at = ((k_hbm, kvt_v.at[0], kv_s), (v_hbm, kvt_v.at[1], kv_s), (q_hbm, qgo_v.at[0], x_s), (g_hbm, qgo_v.at[1], x_s))
    for src, dst, sem in (*heads_at, (o_hbm, qgo_v.at[2], x_s), (l_hbm, l_v, r_s), (ch_hbm, ch_v, p_s), (x_hbm, xg.at[x], y_s)):
        pltpu.make_async_copy(src, dst, sem).start()
    taken(kvt_v, kv_s)
    tok, heads = qgo_v.shape[1], qgo_v.shape[2] // DH
    nb = tok // BLOCK
    width = heads * BLOCK
    reach = [1, total // 8, total // 4, total // 2]
    kv_v[...] = kvt_v[...].reshape(2 * DH, tok).T
    pl.semaphore_wait(barrier, peers)

    sends_to = [me + r < total for r in reach]
    gets_from = [me >= r for r in reach]
    kv_out = [
        remote(kv_v, far.at[0], kv_s, kv_r.at[0], segment(me + reach[0])),
        remote(kv_v, far.at[1], kv_s, kv_r.at[1], zmate(step // 2)),
        remote(far.at[1], far.at[2], kv_s, kv_r.at[2], zmate(step // 2)),
        remote(far.at[2], far.at[3], kv_s, kv_r.at[3], zmate(step)),
        remote(kv_v, far.at[4], kv_s, kv_r.at[3], zmate(-step)),
        remote(far.at[4], far.at[3], kv_s, kv_r.at[3], zmate(-step)),
    ]
    goes = sends_to[:2] + [
        jnp.logical_and(z >= step // 2, z + step // 2 < nz),
        jnp.logical_and(z >= step, z < 2 * step),
        jnp.logical_and(z >= step, z < 2 * step),
        z < step,
    ]

    def pass_on(l):
        @pl.when(goes[l])
        def _():
            kv_out[l].start()

    pass_on(0)
    pass_on(1)
    pass_on(4)

    def hello(sem, device):
        pl.semaphore_signal(sem, inc=1, device_id=device, device_id_type=MESH)

    @pl.when(jnp.logical_and(late, z < last))
    def _():
        hello(near_sem.at[0], zmate(-step))

    @pl.when(z >= last)
    def _():
        hello(near_sem.at[1], zmate(step))

    @pl.when(z == nz - 2)
    def _():
        hello(near_sem.at[2], zmate(-2))

    @pl.when(z == nz - 1)
    def _():
        hello(near_sem.at[2], zmate(1))

    for d in (2, -2):
        hello(near_sem.at[3], at(z, lax.rem(y + d + ny, ny), c, x))

    x_out = [
        remote(xg.at[x], xg.at[x], x_s, x_r.at[x], at(z, y, c, lax.rem(x + d, nx))) for d in range(1, nx)
    ]

    taken(qgo_v, x_s)
    taken(xg.at[x], y_s)
    @pl.when(x == 0)
    def _():
        for cp in x_out:
            cp.start()

    taken(l_v, r_s)
    taken(ch_v, p_s)
    q_v, g_v, o_v = (qgo_v.at[i] for i in range(3))

    low = lax.broadcasted_iota(jnp.int32, (BLOCK, 2 * DH), 1) < DH
    for b in range(nb):
        for hp in range(heads // 2):
            rows = pl.ds(b * BLOCK, BLOCK)
            cols = pl.ds(hp * 2 * DH, 2 * DH)
            qt = q_v[rows, cols].astype(F32) * (DH**-0.5)
            gt = g_v[rows, cols].astype(F32)
            qr = pltpu.roll(qt, DH, 1)
            gr = pltpu.roll(gt, DH, 1)
            for k, (qq, gg) in enumerate(((qt, gr), (qr, gt))):
                h = hp * 2 + k
                w_v[b, pl.ds(h * BLOCK, BLOCK), :] = jnp.where(low, qq, 0.0).astype(BF16)
                w_v[b, pl.ds((heads + h) * BLOCK, BLOCK), :] = jnp.where(low, 0.0, gg).astype(BF16)

    prod = g_v[...].astype(F32) * o_v[...].astype(F32)
    delta = jnp.sum(prod.T.reshape(heads, DH, tok), axis=1)
    lse = l_v[...] * LOG2E
    for b in range(nb):
        for h in range(heads):
            cols = pl.ds(h * BLOCK, BLOCK)
            drow[b, :, cols] = delta[h : h + 1, b * BLOCK : (b + 1) * BLOCK]
            lrow[b, :, cols] = lse[h : h + 1, b * BLOCK : (b + 1) * BLOCK]

    lane = lax.broadcasted_iota(jnp.int32, ch_v.shape, 1)
    for b in range(nb):
        sel = jnp.sum(jnp.where(lane == me * nb + b, ch_v[...].astype(F32), 0.0), axis=1, keepdims=True)
        for l in range(LEVELS):
            for k in range(nb):
                want = ((me - reach[l]) * nb + k).astype(F32)
                hit = jnp.max(jnp.where(sel[PER * l : PER * (l + 1)] == want, 1.0, 0.0), axis=0, keepdims=True)
                nrow[l, b, k] = lrow[b] + (1.0 - hit) * BIG

    def first(kv, b):
        return nt(kv, w_v[b, pl.ds(0, width), :]), nt(kv, w_v[b, pl.ds(width, width), :])

    def middle(scores, dprobs, b, l_of, keep):
        dl = drow[b]
        ps, ds = [], []
        for k in range(scores.shape[0] // BLOCK):
            rows = slice(k * BLOCK, (k + 1) * BLOCK)
            p = jnp.exp2(scores[rows] * LOG2E - l_of(k))
            if keep is not None:
                p = jnp.where(keep, p, 0.0)
            ps.append(p.astype(BF16))
            ds.append((p * (dprobs[rows] - dl)).astype(BF16))
        return jnp.concatenate([jnp.concatenate(ds, axis=0), jnp.concatenate(ps, axis=0)], axis=1)

    def second(kv, b, dp):
        return nn(dp, w_v[b]), tn(kv[:, :DH], dp[:, :width])

    def tile(kv, b, l_of, keep):
        return second(kv, b, middle(*first(kv, b), b, l_of, keep))

    keep = lax.broadcasted_iota(jnp.int32, (BLOCK, width), 0) <= lax.rem(
        lax.broadcasted_iota(jnp.int32, (BLOCK, width), 1), BLOCK
    )
    for b in range(nb):
        rows = pl.ds(b * BLOCK, BLOCK)
        dkv, dq = tile(kv_v[rows, :], b, lambda k: lrow[b], keep)
        dkv_own[rows, :] = dkv
        dqt[b] = dq

    @pl.when(x != 0)
    def _():
        for cp in x_out:
            cp.start()

    def arrived(l):
        @pl.when(gets_from[l])
        def _():
            taken(far.at[l], kv_r.at[l])

    arrived(1)
    pass_on(2)

    def terms(l):
        kv = far[l]
        raw = [first(kv, b) for b in range(nb)]
        dps = [middle(*raw[b], b, lambda k, b=b: nrow[l, b, k], None) for b in range(nb)]
        for b in range(nb):
            dqt[b] = dqt[b] + tn(kv[:, :DH], dps[b][:, :width])
        return jnp.concatenate(dps, axis=1)

    def toward_keys(l, dps):
        back[l] = nn(dps, w_v[...].reshape(nb * 2 * width, 2 * DH)).astype(BF16)

    def level(l):
        toward_keys(l, terms(l))

    ret_out = [remote(back.at[l], ret.at[l], r_s, r_r, segment(me - reach[l])) for l in range(LEVELS)]

    def run_level(l):
        @pl.when(gets_from[l])
        def _():
            level(l)

    def give_back(l):
        @pl.when(gets_from[l])
        def _():
            ret_out[l].start()

    def flip(b):
        for k in range(step):
            xt[b * step + k] = xg[b, :, pl.ds(k * 128, 128)].T

    def block_of_x(b):
        @pl.when(x != b)
        def _():
            taken(xg.at[b], x_r.at[b])

        flip(b)

    run_level(1)
    arrived(0)
    run_level(0)
    arrived(2)

    @pl.when(goes[3])
    def _():
        pl.semaphore_wait(near_sem.at[0], 1)
        kv_out[3].start()
        hello(near_sem.at[0], zmate(-step))

    give_back(1)
    give_back(0)
    run_level(2)
    give_back(2)

    arrived(3)

    @pl.when(late)
    def _():
        dp_v[...] = terms(3)

    @pl.when(goes[5])
    def _():
        pl.semaphore_wait(near_sem.at[1], 1)
        taken(far.at[4], kv_r.at[3])
        kv_out[5].start()

    block_of_x(0)

    for b in range(nb):
        t = (dqt[b] * (DH**-0.5)).astype(BF16).T
        for h in range(heads):
            dq_ref[pl.ds(b * BLOCK, BLOCK), pl.ds(h * DH, DH)] = t[h * BLOCK : (h + 1) * BLOCK]
    dq = dq_ref[...]

    feats = 128

    def product(z0, n):
        return nn(xt[pl.ds(z0, n)].reshape(n * feats, tok), dq)

    def rows_of(g):
        z0, n = groups[g]
        return pl.ds(z0, n)

    def pair(g):
        z0, n = groups[g]

        def one(i, carry):
            part = product(z0 + i, 1).reshape(ny, nc, feats // seats, width).astype(BF16)
            for e in range(nc):
                pe[e, z0 + i] = part[:, e]
            return carry

        lax.fori_loop(0, n, one, 0, unroll=n <= 2)
        rows = rows_of(g)
        remote(pe.at[1 - c, rows], pr.at[rows], p_s, p_r.at[g], at(z, y, 1 - c, x)).start()

    def across_y(g):
        rows = rows_of(g)
        taken(pr.at[rows], p_r.at[g])
        for yy in range(ny):
            ys[yy, rows] = (pe[c, rows, yy].astype(F32) + pr[rows, yy].astype(F32)).astype(BF16)
        yr[y, rows] = ys[y, rows]
        for d in sorted(range(1, ny), key=lambda d: -min(d, ny - d)):
            yy = lax.rem(y + d, ny)
            remote(ys.at[yy, rows], yr.at[y, rows], y_s, y_r.at[g], at(z, yy, c, x)).start()

    def to_owner(zz):
        @pl.when(zz != z)
        def _():
            remote(zs.at[zz], zr.at[z], z_s, z_r, at(zz, y, c, x)).start()

        @pl.when(zz == z)
        def _():
            zr[z] = zs[zz]

    def across_z(g):
        z0, n = groups[g]
        rows = rows_of(g)
        taken(yr.at[pl.ds(0, ny - 1), rows], y_r.at[g])
        acc = yr[0, rows].astype(F32)
        for k in range(1, ny):
            acc = acc + yr[k, rows].astype(F32)
        zs[rows] = acc.astype(BF16)
        for i in range(n):
            to_owner(z0 + i)

    @pl.when(jnp.logical_not(late))
    def _():
        pair(0)
        pl.semaphore_wait(near_sem.at[3], 2)
        across_y(0)
        pair(1)
        across_y(1)
        block_of_x(1)
        block_of_x(2)
        block_of_x(3)
        pair(3)
        across_y(3)

        @pl.when(goes[5])
        def _():
            pl.semaphore_wait(near_sem.at[0], 1)

            @pl.when(z == 0)
            def _():
                pl.semaphore_wait(near_sem.at[2], 1)

            hello(near_sem.at[1], zmate(step))

        @pl.when(goes[3])
        def _():
            pl.semaphore_wait(near_sem.at[1], 1)
            hello(near_sem.at[1], zmate(step))

        pair(2)
        across_y(2)
        across_z(0)
        across_z(1)
        across_z(2)
        across_z(3)

    @pl.when(late)
    def _():
        pair(0)
        pair(1)
        pl.semaphore_wait(near_sem.at[3], 2)
        across_y(0)
        across_y(1)
        toward_keys(3, dp_v[...])
        ret_out[3].start()
        block_of_x(1)
        pair(2)
        across_y(2)
        block_of_x(2)
        block_of_x(3)
        pair(3)

        @pl.when(z < last)
        def _():
            pl.semaphore_wait(near_sem.at[1], 1)

        @pl.when(z == last)
        def _():
            pl.semaphore_wait(near_sem.at[2], 1)

        across_z(0)
        across_z(1)
        across_y(3)
        across_z(2)

    def count(flags):
        return sum(f.astype(jnp.int32) for f in flags)

    def slots(ref, sem, number, most):
        for k in range(1, most + 1):

            @pl.when(number == k)
            def _(k=k):
                taken(ref.at[pl.ds(0, k)], sem)

    slots(ret, r_r, count(sends_to), LEVELS)
    for l in range(LEVELS):

        @pl.when(sends_to[l])
        def _(l=l):
            dkv_own[...] = dkv_own[...] + ret[l].astype(F32)

    total_kv = dkv_own[...].T
    dk_ref[...] = total_kv[:DH].astype(BF16)
    dv_ref[...] = total_kv[DH:].astype(BF16)

    @pl.when(late)
    def _():
        across_z(ng - 1)

    slots(far, kv_s, count(goes), LEVELS + 1)
    slots(back, r_s, count(gets_from), LEVELS)
    taken(xg.at[pl.ds(0, nx - 1)], x_s)
    taken(pr, p_s)
    taken(ys.at[pl.ds(0, ny - 1)], y_s)
    taken(zs.at[pl.ds(0, nz - 1)], z_s)
    taken(zr.at[pl.ds(0, nz - 1)], z_r)
    acc = zr[0].astype(F32)
    for k in range(1, nz):
        acc = acc + zr[k].astype(F32)
    dw_ref[...] = acc


def write(dq, dk, dv, dw, dq_out, dk_out, dv_out, dw_out, sem):
    copies = [
        pltpu.make_async_copy(s, d, sem.at[i])
        for i, (s, d) in enumerate(((dq, dq_out), (dk, dk_out), (dv, dv_out), (dw, dw_out)))
    ]
    for cp in copies:
        cp.start()
    for cp in copies:
        cp.wait()


def shards(layer_input, queries, keys, values, attn_out, grad_out, log_sum, chosen):
    nz, ny, nc, nx = (SIZES[a] for a in ("z", "y", "c", "x"))
    total = nz * ny * nc
    tok, qw = queries.shape
    nb = tok // BLOCK
    heads = qw // DH
    feats = layer_input.shape[1]
    rows_out = feats * nx // total
    groups = groups_of(nz)
    ng = len(groups)
    dma = pltpu.SemaphoreType.DMA
    vm = pltpu.VMEM
    hbm = pl.BlockSpec(memory_space=pltpu.HBM)
    vmem = pl.BlockSpec(memory_space=pltpu.VMEM)
    shapes = (
        jax.ShapeDtypeStruct((tok, qw), BF16),
        jax.ShapeDtypeStruct((DH, tok), BF16),
        jax.ShapeDtypeStruct((DH, tok), BF16),
        jax.ShapeDtypeStruct((rows_out, qw), F32),
    )
    parts = pl.pallas_call(
        kernel,
        out_shape=tuple(pltpu.VMEM(s.shape, s.dtype) for s in shapes),
        in_specs=[hbm] * 8,
        out_specs=(vmem,) * 4,
        scratch_shapes=[
            vm((3, tok, qw), BF16), vm((heads, tok), F32), vm((LEVELS * PER, chosen.shape[0]), jnp.int32),
            vm((2, DH, tok), BF16), vm((tok, 2 * DH), BF16),
            vm((nb, 2 * heads * BLOCK, 2 * DH), BF16), vm((tok, nb * 2 * heads * BLOCK), BF16),
            vm((nb, 1, heads * BLOCK), F32),
            vm((LEVELS, nb, nb, 1, heads * BLOCK), F32), vm((nb, 1, heads * BLOCK), F32),
            vm((nb, DH, heads * BLOCK), F32), vm((tok, 2 * DH), F32),
            vm((LEVELS + 1, tok, 2 * DH), BF16), vm((LEVELS, tok, 2 * DH), BF16), vm((LEVELS, tok, 2 * DH), BF16),
            vm((nx, tok, feats), BF16), vm((nz, feats * nx // nz, tok), BF16),
            vm((nc, nz, ny, rows_out, qw), BF16), vm((nz, ny, rows_out, qw), BF16),
            vm((ny, nz, rows_out, qw), BF16), vm((ny, nz, rows_out, qw), BF16),
            vm((nz, rows_out, qw), BF16), vm((nz, rows_out, qw), BF16),
            dma((6,)), dma((LEVELS,)), dma((nx,)), dma, dma((ng,)), dma((ng,)), dma,
            pltpu.SemaphoreType.REGULAR((4,)),
        ],
        compiler_params=pltpu.CompilerParams(collective_id=0, has_side_effects=True, vmem_limit_bytes=48 * 1024 * 1024),
        name="whole",
    )(
        *(
            pltpu.with_memory_space_constraint(a, pltpu.HBM)
            for a in (layer_input, queries, keys.T, values.T, attn_out, grad_out, log_sum.T, chosen.T)
        )
    )
    parts = [pltpu.with_memory_space_constraint(a, pltpu.VMEM) for a in parts]
    dq, dk, dv, dw = pl.pallas_call(
        write,
        out_shape=shapes,
        in_specs=[vmem] * 4,
        out_specs=(hbm,) * 4,
        scratch_shapes=[dma((4,))],
        name="write",
    )(*parts)
    return dq, dk.T, dv.T, dw


def solution(mesh):
    torus = Mesh(
        mesh.devices.reshape(SIZES["z"], SIZES["y"], SIZES["c"], SIZES["x"]), ("z", "y", "c", "x")
    )
    spec = P(KV, "x")
    return jax.shard_map(
        shards,
        mesh=torus,
        in_specs=(spec,) * 7 + (P(),),
        out_specs=(spec,) * 4,
        check_vma=False,
    )
```

```python
import functools

import jax
import jax.numpy as jnp
from jax import lax
from jax.experimental import pallas as pl
from jax.experimental.pallas import tpu as pltpu
from jax.sharding import Mesh
from jax.sharding import PartitionSpec as P

MESH = pl.DeviceIdType.MESH
F32 = jnp.float32
BF16 = jnp.bfloat16

DH = 64
BLOCK = 64
PER = 2
LEVELS = 4
LOG2E = 1.4426950408889634
BIG = 1e30
SIZES = {"z": 16, "y": 8, "c": 2, "x": 4}
KV = ("z", "y", "c")


def nt(a, b):
    return lax.dot_general(a, b, (((1,), (1,)), ((), ())), preferred_element_type=F32)


def tn(a, b):
    return lax.dot_general(a, b, (((0,), (0,)), ((), ())), preferred_element_type=F32)


def nn(a, b):
    return lax.dot_general(a, b, (((1,), (0,)), ((), ())), preferred_element_type=F32)


def groups_of(end):
    cuts = [0, 2, 4, end // 2, end]
    return [(a, b - a) for a, b in zip(cuts, cuts[1:])]


def kernel(
    x_hbm, q_hbm, k_hbm, v_hbm, o_hbm, g_hbm, l_hbm, ch_hbm,
    dq_ref, dk_ref, dv_ref, dw_ref,
    qgo_v, l_v, ch_v, kvt_v, kv_v,
    w_v, dp_v, lrow, nrow, drow, dqt, dkv_own, far, back, ret,
    xg, xt, *rest,
):
    nz, ny, nc, nx = (SIZES[a] for a in ("z", "y", "c", "x"))
    groups = groups_of(nz)
    ng = len(groups)
    pe, pr, ys, yr, zs, zr, sent, kv_r, x_r, r_r, p_r, y_r, z_r, near_sem = rest
    kv_s, x_s, r_s, p_s, y_s, z_s = (sent.at[i] for i in range(6))
    z, y, c, x = (lax.axis_index(a) for a in ("z", "y", "c", "x"))
    total = nz * ny * nc
    me = (z * ny + y) * nc + c
    seat = y * nc + c
    seats = ny * nc
    step = nz // 4

    def at(zz, yy, cc, xx):
        return {"z": zz, "y": yy, "c": cc, "x": xx}

    def zmate(d):
        return at(lax.rem(z + d + nz, nz), y, c, x)

    def segment(s):
        return at(s // (ny * nc), lax.rem(s // nc, ny), lax.rem(s, nc), x)

    def remote(src, dst, ssem, rsem, device):
        return pltpu.make_async_remote_copy(
            src_ref=src, dst_ref=dst, send_sem=ssem, recv_sem=rsem, device_id=device, device_id_type=MESH
        )

    def taken(ref, sem):
        pltpu.make_async_copy(ref, ref, sem).wait()

    barrier = pltpu.get_barrier_semaphore()

    def tell(device):
        pl.semaphore_signal(barrier, inc=1, device_id=device, device_id_type=MESH)

    late = z >= nz // 2
    last = nz - step
    for d in range(step, 0, -1):
        below, above = zmate(-d), zmate(d)
        if d <= step // 2:
            tell(below)
        else:

            @pl.when(z < d)
            def _(below=below):
                tell(below)

        @pl.when(z + d < nz if d <= step // 2 else jnp.logical_and(z + d < nz, jnp.logical_not(late)))
        def _(above=above):
            tell(above)

    beside = jnp.int32(0)
    for d in range(1, step + 1):
        near = d <= step // 2
        beside += jnp.where(jnp.logical_and(z >= d, jnp.logical_or(near, z - d < nz // 2)), 1, 0)
        beside += jnp.where(jnp.logical_or(z + d >= nz, near), 1, 0) * jnp.where(
            jnp.logical_or(z + d < nz, z >= last), 1, 0
        )

    up = jnp.logical_and(jnp.logical_and(y == ny - 1, c == nc - 1), z < nz - 1)
    down = jnp.logical_and(seat == 0, z > 0)

    @pl.when(up)
    def _():
        tell(segment(me + 1))

    @pl.when(down)
    def _():
        tell(segment(me - 1))

    for d in range(1, nx):
        tell(at(z, y, c, lax.rem(x + d, nx)))

    tell(at(z, y, 1 - c, x))
    for d in (2, 1):
        for e in range(nc):
            tell(at(z, lax.rem(y + d, ny), e, x))
            tell(at(z, lax.rem(y + ny - d, ny), e, x))
    peers = beside + nx - 1 + 1 + 4 * nc + up.astype(jnp.int32) + down.astype(jnp.int32)

    heads_at = ((k_hbm, kvt_v.at[0], kv_s), (v_hbm, kvt_v.at[1], kv_s), (q_hbm, qgo_v.at[0], x_s), (g_hbm, qgo_v.at[1], x_s))
    for src, dst, sem in (*heads_at, (o_hbm, qgo_v.at[2], x_s), (l_hbm, l_v, r_s), (ch_hbm, ch_v, p_s), (x_hbm, xg.at[x], y_s)):
        pltpu.make_async_copy(src, dst, sem).start()
    taken(kvt_v, kv_s)
    tok, heads = qgo_v.shape[1], qgo_v.shape[2] // DH
    nb = tok // BLOCK
    width = heads * BLOCK
    reach = [1, total // 8, total // 4, total // 2]
    kv_v[...] = kvt_v[...].reshape(2 * DH, tok).T
    pl.semaphore_wait(barrier, peers)

    sends_to = [me + r < total for r in reach]
    gets_from = [me >= r for r in reach]
    kv_out = [
        remote(kv_v, far.at[0], kv_s, kv_r.at[0], segment(me + reach[0])),
        remote(kv_v, far.at[1], kv_s, kv_r.at[1], zmate(step // 2)),
        remote(far.at[1], far.at[2], kv_s, kv_r.at[2], zmate(step // 2)),
        remote(far.at[2], far.at[3], kv_s, kv_r.at[3], zmate(step)),
        remote(kv_v, far.at[4], kv_s, kv_r.at[3], zmate(-step)),
        remote(far.at[4], far.at[3], kv_s, kv_r.at[3], zmate(-step)),
    ]
    goes = sends_to[:2] + [
        jnp.logical_and(z >= step // 2, z + step // 2 < nz),
        jnp.logical_and(z >= step, z < 2 * step),
        jnp.logical_and(z >= step, z < 2 * step),
        z < step,
    ]

    def pass_on(l):
        @pl.when(goes[l])
        def _():
            kv_out[l].start()


    def hello(sem, device):
        pl.semaphore_signal(sem, inc=1, device_id=device, device_id_type=MESH)

    @pl.when(jnp.logical_and(late, z < last))
    def _():
        hello(near_sem.at[0], zmate(-step))

    @pl.when(z >= last)
    def _():
        hello(near_sem.at[1], zmate(step))

    @pl.when(z == nz - 2)
    def _():
        hello(near_sem.at[2], zmate(-2))

    @pl.when(z == nz - 1)
    def _():
        hello(near_sem.at[2], zmate(1))

    pass_on(0)
    pass_on(1)
    pass_on(4)

    for d in (2, -2):
        hello(near_sem.at[3], at(z, lax.rem(y + d + ny, ny), c, x))

    x_out = [
        remote(xg.at[x], xg.at[x], x_s, x_r.at[x], at(z, y, c, lax.rem(x + d, nx))) for d in range(1, nx)
    ]

    taken(qgo_v, x_s)
    taken(xg.at[x], y_s)
    @pl.when(x == 0)
    def _():
        for cp in x_out:
            cp.start()

    taken(l_v, r_s)
    taken(ch_v, p_s)
    q_v, g_v, o_v = (qgo_v.at[i] for i in range(3))

    low = lax.broadcasted_iota(jnp.int32, (BLOCK, 2 * DH), 1) < DH
    for b in range(nb):
        for hp in range(heads // 2):
            rows = pl.ds(b * BLOCK, BLOCK)
            cols = pl.ds(hp * 2 * DH, 2 * DH)
            qt = q_v[rows, cols].astype(F32) * (DH**-0.5)
            gt = g_v[rows, cols].astype(F32)
            qr = pltpu.roll(qt, DH, 1)
            gr = pltpu.roll(gt, DH, 1)
            for k, (qq, gg) in enumerate(((qt, gr), (qr, gt))):
                h = hp * 2 + k
                w_v[b, pl.ds(h * BLOCK, BLOCK), :] = jnp.where(low, qq, 0.0).astype(BF16)
                w_v[b, pl.ds((heads + h) * BLOCK, BLOCK), :] = jnp.where(low, 0.0, gg).astype(BF16)

    prod = g_v[...].astype(F32) * o_v[...].astype(F32)
    delta = jnp.sum(prod.T.reshape(heads, DH, tok), axis=1)
    lse = l_v[...] * LOG2E
    for b in range(nb):
        for h in range(heads):
            cols = pl.ds(h * BLOCK, BLOCK)
            drow[b, :, cols] = delta[h : h + 1, b * BLOCK : (b + 1) * BLOCK]
            lrow[b, :, cols] = lse[h : h + 1, b * BLOCK : (b + 1) * BLOCK]

    lane = lax.broadcasted_iota(jnp.int32, ch_v.shape, 1)
    for b in range(nb):
        sel = jnp.sum(jnp.where(lane == me * nb + b, ch_v[...].astype(F32), 0.0), axis=1, keepdims=True)
        for l in range(LEVELS):
            for k in range(nb):
                want = ((me - reach[l]) * nb + k).astype(F32)
                hit = jnp.max(jnp.where(sel[PER * l : PER * (l + 1)] == want, 1.0, 0.0), axis=0, keepdims=True)
                nrow[l, b, k] = lrow[b] + (1.0 - hit) * BIG

    def first(kv, b):
        return nt(kv, w_v[b, pl.ds(0, width), :]), nt(kv, w_v[b, pl.ds(width, width), :])

    def middle(scores, dprobs, b, l_of, keep):
        dl = drow[b]
        ps, ds = [], []
        for k in range(scores.shape[0] // BLOCK):
            rows = slice(k * BLOCK, (k + 1) * BLOCK)
            p = jnp.exp2(scores[rows] * LOG2E - l_of(k))
            if keep is not None:
                p = jnp.where(keep, p, 0.0)
            ps.append(p.astype(BF16))
            ds.append((p * (dprobs[rows] - dl)).astype(BF16))
        return jnp.concatenate([jnp.concatenate(ds, axis=0), jnp.concatenate(ps, axis=0)], axis=1)

    def second(kv, b, dp):
        return nn(dp, w_v[b]), tn(kv[:, :DH], dp[:, :width])

    def tile(kv, b, l_of, keep):
        return second(kv, b, middle(*first(kv, b), b, l_of, keep))

    keep = lax.broadcasted_iota(jnp.int32, (BLOCK, width), 0) <= lax.rem(
        lax.broadcasted_iota(jnp.int32, (BLOCK, width), 1), BLOCK
    )
    for b in range(nb):
        rows = pl.ds(b * BLOCK, BLOCK)
        dkv, dq = tile(kv_v[rows, :], b, lambda k: lrow[b], keep)
        dkv_own[rows, :] = dkv
        dqt[b] = dq

    @pl.when(x != 0)
    def _():
        for cp in x_out:
            cp.start()

    def arrived(l):
        @pl.when(gets_from[l])
        def _():
            taken(far.at[l], kv_r.at[l])

    arrived(1)
    pass_on(2)

    def terms(l):
        kv = far[l]
        raw = [first(kv, b) for b in range(nb)]
        dps = [middle(*raw[b], b, lambda k, b=b: nrow[l, b, k], None) for b in range(nb)]
        for b in range(nb):
            dqt[b] = dqt[b] + tn(kv[:, :DH], dps[b][:, :width])
        return jnp.concatenate(dps, axis=1)

    def toward_keys(l, dps):
        back[l] = nn(dps, w_v[...].reshape(nb * 2 * width, 2 * DH)).astype(BF16)

    def level(l):
        toward_keys(l, terms(l))

    ret_out = [remote(back.at[l], ret.at[l], r_s, r_r, segment(me - reach[l])) for l in range(LEVELS)]

    def run_level(l):
        @pl.when(gets_from[l])
        def _():
            level(l)

    def give_back(l):
        @pl.when(gets_from[l])
        def _():
            ret_out[l].start()

    def flip(b):
        for k in range(step):
            xt[b * step + k] = xg[b, :, pl.ds(k * 128, 128)].T

    def block_of_x(b):
        @pl.when(x != b)
        def _():
            taken(xg.at[b], x_r.at[b])

        flip(b)

    run_level(1)
    arrived(0)
    run_level(0)
    arrived(2)

    @pl.when(goes[3])
    def _():
        pl.semaphore_wait(near_sem.at[0], 1)
        kv_out[3].start()
        hello(near_sem.at[0], zmate(-step))

    give_back(1)
    give_back(0)
    run_level(2)
    give_back(2)

    arrived(3)

    @pl.when(late)
    def _():
        dp_v[...] = terms(3)

    @pl.when(goes[5])
    def _():
        pl.semaphore_wait(near_sem.at[1], 1)
        taken(far.at[4], kv_r.at[3])
        kv_out[5].start()

    block_of_x(0)

    for b in range(nb):
        t = (dqt[b] * (DH**-0.5)).astype(BF16).T
        for h in range(heads):
            dq_ref[pl.ds(b * BLOCK, BLOCK), pl.ds(h * DH, DH)] = t[h * BLOCK : (h + 1) * BLOCK]
    dq = dq_ref[...]

    feats = 128

    def product(z0, n):
        return nn(xt[pl.ds(z0, n)].reshape(n * feats, tok), dq)

    def rows_of(g):
        z0, n = groups[g]
        return pl.ds(z0, n)

    def pair(g):
        z0, n = groups[g]

        def one(i, carry):
            part = product(z0 + i, 1).reshape(ny, nc, feats // seats, width).astype(BF16)
            for e in range(nc):
                pe[e, z0 + i] = part[:, e]
            return carry

        lax.fori_loop(0, n, one, 0, unroll=n <= 2)
        rows = rows_of(g)
        remote(pe.at[1 - c, rows], pr.at[rows], p_s, p_r.at[g], at(z, y, 1 - c, x)).start()

    def across_y(g):
        rows = rows_of(g)
        taken(pr.at[rows], p_r.at[g])
        for yy in range(ny):
            ys[yy, rows] = (pe[c, rows, yy].astype(F32) + pr[rows, yy].astype(F32)).astype(BF16)
        yr[y, rows] = ys[y, rows]
        for d in sorted(range(1, ny), key=lambda d: -min(d, ny - d)):
            yy = lax.rem(y + d, ny)
            remote(ys.at[yy, rows], yr.at[y, rows], y_s, y_r.at[g], at(z, yy, c, x)).start()

    def to_owner(zz):
        @pl.when(zz != z)
        def _():
            remote(zs.at[zz], zr.at[z], z_s, z_r, at(zz, y, c, x)).start()

        @pl.when(zz == z)
        def _():
            zr[z] = zs[zz]

    def across_z(g):
        z0, n = groups[g]
        rows = rows_of(g)
        taken(yr.at[pl.ds(0, ny - 1), rows], y_r.at[g])
        for i in range(n):
            acc = yr[0, z0 + i].astype(F32)
            for k in range(1, ny):
                acc = acc + yr[k, z0 + i].astype(F32)
            zs[z0 + i] = acc.astype(BF16)
            to_owner(z0 + i)

    @pl.when(jnp.logical_not(late))
    def _():
        pair(0)
        pl.semaphore_wait(near_sem.at[3], 2)
        across_y(0)
        pair(1)
        across_y(1)
        block_of_x(1)
        block_of_x(2)
        block_of_x(3)
        pair(3)
        across_y(3)

        @pl.when(goes[5])
        def _():
            pl.semaphore_wait(near_sem.at[0], 1)

            @pl.when(z == 0)
            def _():
                pl.semaphore_wait(near_sem.at[2], 1)

            hello(near_sem.at[1], zmate(step))

        @pl.when(goes[3])
        def _():
            pl.semaphore_wait(near_sem.at[1], 1)
            hello(near_sem.at[1], zmate(step))

        pair(2)
        across_y(2)
        across_z(0)
        across_z(1)
        across_z(2)
        across_z(3)

    @pl.when(late)
    def _():
        pair(0)
        pl.semaphore_wait(near_sem.at[3], 2)

        @pl.when(c != nc - 1)
        def _():
            across_y(0)
            pair(1)

        @pl.when(c == nc - 1)
        def _():
            pair(1)
            across_y(0)

        across_y(1)
        toward_keys(3, dp_v[...])
        ret_out[3].start()
        block_of_x(1)
        pair(2)
        across_y(2)
        block_of_x(2)
        block_of_x(3)
        pair(3)

        @pl.when(z < last)
        def _():
            pl.semaphore_wait(near_sem.at[1], 1)

        @pl.when(z == last)
        def _():
            pl.semaphore_wait(near_sem.at[2], 1)

        across_z(0)
        across_z(1)
        across_y(3)
        across_z(2)

    def count(flags):
        return sum(f.astype(jnp.int32) for f in flags)

    def slots(ref, sem, number, most):
        for k in range(1, most + 1):

            @pl.when(number == k)
            def _(k=k):
                taken(ref.at[pl.ds(0, k)], sem)

    slots(ret, r_r, count(sends_to), LEVELS)
    for l in range(LEVELS):

        @pl.when(sends_to[l])
        def _(l=l):
            dkv_own[...] = dkv_own[...] + ret[l].astype(F32)

    total_kv = dkv_own[...].T
    dk_ref[...] = total_kv[:DH].astype(BF16)
    dv_ref[...] = total_kv[DH:].astype(BF16)

    @pl.when(late)
    def _():
        across_z(ng - 1)

    slots(far, kv_s, count(goes), LEVELS + 1)
    slots(back, r_s, count(gets_from), LEVELS)
    taken(xg.at[pl.ds(0, nx - 1)], x_s)
    taken(pr, p_s)
    taken(ys.at[pl.ds(0, ny - 1)], y_s)
    taken(zs.at[pl.ds(0, nz - 1)], z_s)
    taken(zr.at[pl.ds(0, nz - 1)], z_r)
    acc = zr[0].astype(F32)
    for k in range(1, nz):
        acc = acc + zr[k].astype(F32)
    dw_ref[...] = acc


def write(dq, dk, dv, dw, dq_out, dk_out, dv_out, dw_out, sem):
    copies = [
        pltpu.make_async_copy(s, d, sem.at[i])
        for i, (s, d) in enumerate(((dq, dq_out), (dk, dk_out), (dv, dv_out), (dw, dw_out)))
    ]
    for cp in copies:
        cp.start()
    for cp in copies:
        cp.wait()


def shards(layer_input, queries, keys, values, attn_out, grad_out, log_sum, chosen):
    nz, ny, nc, nx = (SIZES[a] for a in ("z", "y", "c", "x"))
    total = nz * ny * nc
    tok, qw = queries.shape
    nb = tok // BLOCK
    heads = qw // DH
    feats = layer_input.shape[1]
    rows_out = feats * nx // total
    groups = groups_of(nz)
    ng = len(groups)
    dma = pltpu.SemaphoreType.DMA
    vm = pltpu.VMEM
    hbm = pl.BlockSpec(memory_space=pltpu.HBM)
    vmem = pl.BlockSpec(memory_space=pltpu.VMEM)
    shapes = (
        jax.ShapeDtypeStruct((tok, qw), BF16),
        jax.ShapeDtypeStruct((DH, tok), BF16),
        jax.ShapeDtypeStruct((DH, tok), BF16),
        jax.ShapeDtypeStruct((rows_out, qw), F32),
    )
    parts = pl.pallas_call(
        kernel,
        out_shape=tuple(pltpu.VMEM(s.shape, s.dtype) for s in shapes),
        in_specs=[hbm] * 8,
        out_specs=(vmem,) * 4,
        scratch_shapes=[
            vm((3, tok, qw), BF16), vm((heads, tok), F32), vm((LEVELS * PER, chosen.shape[0]), jnp.int32),
            vm((2, DH, tok), BF16), vm((tok, 2 * DH), BF16),
            vm((nb, 2 * heads * BLOCK, 2 * DH), BF16), vm((tok, nb * 2 * heads * BLOCK), BF16),
            vm((nb, 1, heads * BLOCK), F32),
            vm((LEVELS, nb, nb, 1, heads * BLOCK), F32), vm((nb, 1, heads * BLOCK), F32),
            vm((nb, DH, heads * BLOCK), F32), vm((tok, 2 * DH), F32),
            vm((LEVELS + 1, tok, 2 * DH), BF16), vm((LEVELS, tok, 2 * DH), BF16), vm((LEVELS, tok, 2 * DH), BF16),
            vm((nx, tok, feats), BF16), vm((nz, feats * nx // nz, tok), BF16),
            vm((nc, nz, ny, rows_out, qw), BF16), vm((nz, ny, rows_out, qw), BF16),
            vm((ny, nz, rows_out, qw), BF16), vm((ny, nz, rows_out, qw), BF16),
            vm((nz, rows_out, qw), BF16), vm((nz, rows_out, qw), BF16),
            dma((6,)), dma((LEVELS,)), dma((nx,)), dma, dma((ng,)), dma((ng,)), dma,
            pltpu.SemaphoreType.REGULAR((4,)),
        ],
        compiler_params=pltpu.CompilerParams(collective_id=0, has_side_effects=True, vmem_limit_bytes=48 * 1024 * 1024),
        name="whole",
    )(
        *(
            pltpu.with_memory_space_constraint(a, pltpu.HBM)
            for a in (layer_input, queries, keys.T, values.T, attn_out, grad_out, log_sum.T, chosen.T)
        )
    )
    parts = [pltpu.with_memory_space_constraint(a, pltpu.VMEM) for a in parts]
    dq, dk, dv, dw = pl.pallas_call(
        write,
        out_shape=shapes,
        in_specs=[vmem] * 4,
        out_specs=(hbm,) * 4,
        scratch_shapes=[dma((4,))],
        name="write",
    )(*parts)
    return dq, dk.T, dv.T, dw


def solution(mesh):
    torus = Mesh(
        mesh.devices.reshape(SIZES["z"], SIZES["y"], SIZES["c"], SIZES["x"]), ("z", "y", "c", "x")
    )
    spec = P(KV, "x")
    return jax.shard_map(
        shards,
        mesh=torus,
        in_specs=(spec,) * 7 + (P(),),
        out_specs=(spec,) * 4,
        check_vma=False,
    )
```

```python
import functools

import jax
import jax.numpy as jnp
from jax import lax
from jax.experimental import pallas as pl
from jax.experimental.pallas import tpu as pltpu
from jax.sharding import Mesh
from jax.sharding import PartitionSpec as P

MESH = pl.DeviceIdType.MESH
F32 = jnp.float32
BF16 = jnp.bfloat16

DH = 64
BLOCK = 64
PER = 2
LEVELS = 4
LOG2E = 1.4426950408889634
BIG = 1e30
SIZES = {"z": 16, "y": 8, "c": 2, "x": 4}
KV = ("z", "y", "c")


def nt(a, b):
    return lax.dot_general(a, b, (((1,), (1,)), ((), ())), preferred_element_type=F32)


def tn(a, b):
    return lax.dot_general(a, b, (((0,), (0,)), ((), ())), preferred_element_type=F32)


def nn(a, b):
    return lax.dot_general(a, b, (((1,), (0,)), ((), ())), preferred_element_type=F32)


def groups_of(end):
    cuts = [0, 2, 4, end // 2, end]
    return [(a, b - a) for a, b in zip(cuts, cuts[1:])]


def kernel(
    x_hbm, q_hbm, k_hbm, v_hbm, o_hbm, g_hbm, l_hbm, ch_hbm,
    dq_ref, dk_ref, dv_ref, dw_ref,
    qgo_v, l_v, ch_v, kvt_v, kv_v,
    w_v, dp_v, lrow, nrow, drow, dqt, dkv_own, far, back, ret,
    xg, xt, *rest,
):
    nz, ny, nc, nx = (SIZES[a] for a in ("z", "y", "c", "x"))
    groups = groups_of(nz)
    ng = len(groups)
    pe, pr, ys, yr, zs, zr, sent, kv_r, x_r, r_r, p_r, y_r, z_r, near_sem = rest
    kv_s, x_s, r_s, p_s, y_s, z_s = (sent.at[i] for i in range(6))
    z, y, c, x = (lax.axis_index(a) for a in ("z", "y", "c", "x"))
    total = nz * ny * nc
    me = (z * ny + y) * nc + c
    seat = y * nc + c
    seats = ny * nc
    step = nz // 4

    def at(zz, yy, cc, xx):
        return {"z": zz, "y": yy, "c": cc, "x": xx}

    def zmate(d):
        return at(lax.rem(z + d + nz, nz), y, c, x)

    def segment(s):
        return at(s // (ny * nc), lax.rem(s // nc, ny), lax.rem(s, nc), x)

    def remote(src, dst, ssem, rsem, device):
        return pltpu.make_async_remote_copy(
            src_ref=src, dst_ref=dst, send_sem=ssem, recv_sem=rsem, device_id=device, device_id_type=MESH
        )

    def taken(ref, sem):
        pltpu.make_async_copy(ref, ref, sem).wait()

    barrier = pltpu.get_barrier_semaphore()

    def tell(device):
        pl.semaphore_signal(barrier, inc=1, device_id=device, device_id_type=MESH)

    late = z >= nz // 2
    last = nz - step
    for d in range(step, 0, -1):
        below, above = zmate(-d), zmate(d)
        if d <= step // 2:
            tell(below)
        else:

            @pl.when(z < d)
            def _(below=below):
                tell(below)

        @pl.when(z + d < nz if d <= step // 2 else jnp.logical_and(z + d < nz, jnp.logical_not(late)))
        def _(above=above):
            tell(above)

    beside = jnp.int32(0)
    for d in range(1, step + 1):
        near = d <= step // 2
        beside += jnp.where(jnp.logical_and(z >= d, jnp.logical_or(near, z - d < nz // 2)), 1, 0)
        beside += jnp.where(jnp.logical_or(z + d >= nz, near), 1, 0) * jnp.where(
            jnp.logical_or(z + d < nz, z >= last), 1, 0
        )

    up = jnp.logical_and(jnp.logical_and(y == ny - 1, c == nc - 1), z < nz - 1)
    down = jnp.logical_and(seat == 0, z > 0)

    @pl.when(up)
    def _():
        tell(segment(me + 1))

    @pl.when(down)
    def _():
        tell(segment(me - 1))

    for d in range(1, nx):
        tell(at(z, y, c, lax.rem(x + d, nx)))

    tell(at(z, y, 1 - c, x))
    for d in (2, 1):
        for e in range(nc):
            tell(at(z, lax.rem(y + d, ny), e, x))
            tell(at(z, lax.rem(y + ny - d, ny), e, x))
    peers = beside + nx - 1 + 1 + 4 * nc + up.astype(jnp.int32) + down.astype(jnp.int32)

    heads_at = ((k_hbm, kvt_v.at[0], kv_s), (v_hbm, kvt_v.at[1], kv_s), (q_hbm, qgo_v.at[0], x_s), (g_hbm, qgo_v.at[1], x_s))
    for src, dst, sem in (*heads_at, (o_hbm, qgo_v.at[2], x_s), (l_hbm, l_v, r_s), (ch_hbm, ch_v, p_s), (x_hbm, xg.at[x], y_s)):
        pltpu.make_async_copy(src, dst, sem).start()
    taken(kvt_v, kv_s)
    tok, heads = qgo_v.shape[1], qgo_v.shape[2] // DH
    nb = tok // BLOCK
    width = heads * BLOCK
    reach = [1, total // 8, total // 4, total // 2]
    kv_v[...] = kvt_v[...].reshape(2 * DH, tok).T
    pl.semaphore_wait(barrier, peers)

    sends_to = [me + r < total for r in reach]
    gets_from = [me >= r for r in reach]
    kv_out = [
        remote(kv_v, far.at[0], kv_s, kv_r.at[0], segment(me + reach[0])),
        remote(kv_v, far.at[1], kv_s, kv_r.at[1], zmate(step // 2)),
        remote(far.at[1], far.at[2], kv_s, kv_r.at[2], zmate(step // 2)),
        remote(far.at[2], far.at[3], kv_s, kv_r.at[3], zmate(step)),
        remote(kv_v, far.at[4], kv_s, kv_r.at[3], zmate(-step)),
        remote(far.at[4], far.at[3], kv_s, kv_r.at[3], zmate(-step)),
    ]
    goes = sends_to[:2] + [
        jnp.logical_and(z >= step // 2, z + step // 2 < nz),
        jnp.logical_and(z >= step, z < 2 * step),
        jnp.logical_and(z >= step, z < 2 * step),
        z < step,
    ]

    def pass_on(l):
        @pl.when(goes[l])
        def _():
            kv_out[l].start()

    pass_on(0)
    pass_on(1)
    pass_on(4)

    def hello(sem, device):
        pl.semaphore_signal(sem, inc=1, device_id=device, device_id_type=MESH)

    @pl.when(jnp.logical_and(late, z < last))
    def _():
        hello(near_sem.at[0], zmate(-step))

    @pl.when(z >= last)
    def _():
        hello(near_sem.at[1], zmate(step))

    @pl.when(z == nz - 2)
    def _():
        hello(near_sem.at[2], zmate(-2))

    @pl.when(z == nz - 1)
    def _():
        hello(near_sem.at[2], zmate(1))

    for d in (2, -2):
        hello(near_sem.at[3], at(z, lax.rem(y + d + ny, ny), c, x))

    x_out = [
        remote(xg.at[x], xg.at[x], x_s, x_r.at[x], at(z, y, c, lax.rem(x + d, nx))) for d in range(1, nx)
    ]

    taken(qgo_v, x_s)
    taken(xg.at[x], y_s)
    @pl.when(x == 0)
    def _():
        for cp in x_out:
            cp.start()

    taken(l_v, r_s)
    taken(ch_v, p_s)
    q_v, g_v, o_v = (qgo_v.at[i] for i in range(3))

    low = lax.broadcasted_iota(jnp.int32, (BLOCK, 2 * DH), 1) < DH
    for b in range(nb):
        for hp in range(heads // 2):
            rows = pl.ds(b * BLOCK, BLOCK)
            cols = pl.ds(hp * 2 * DH, 2 * DH)
            qt = q_v[rows, cols].astype(F32) * (DH**-0.5)
            gt = g_v[rows, cols].astype(F32)
            qr = pltpu.roll(qt, DH, 1)
            gr = pltpu.roll(gt, DH, 1)
            for k, (qq, gg) in enumerate(((qt, gr), (qr, gt))):
                h = hp * 2 + k
                w_v[b, pl.ds(h * BLOCK, BLOCK), :] = jnp.where(low, qq, 0.0).astype(BF16)
                w_v[b, pl.ds((heads + h) * BLOCK, BLOCK), :] = jnp.where(low, 0.0, gg).astype(BF16)

    prod = g_v[...].astype(F32) * o_v[...].astype(F32)
    delta = jnp.sum(prod.T.reshape(heads, DH, tok), axis=1)
    lse = l_v[...] * LOG2E
    for b in range(nb):
        for h in range(heads):
            cols = pl.ds(h * BLOCK, BLOCK)
            drow[b, :, cols] = delta[h : h + 1, b * BLOCK : (b + 1) * BLOCK]
            lrow[b, :, cols] = lse[h : h + 1, b * BLOCK : (b + 1) * BLOCK]

    lane = lax.broadcasted_iota(jnp.int32, ch_v.shape, 1)
    for b in range(nb):
        sel = jnp.sum(jnp.where(lane == me * nb + b, ch_v[...].astype(F32), 0.0), axis=1, keepdims=True)
        for l in range(LEVELS):
            for k in range(nb):
                want = ((me - reach[l]) * nb + k).astype(F32)
                hit = jnp.max(jnp.where(sel[PER * l : PER * (l + 1)] == want, 1.0, 0.0), axis=0, keepdims=True)
                nrow[l, b, k] = lrow[b] + (1.0 - hit) * BIG

    def first(kv, b):
        return nt(kv, w_v[b, pl.ds(0, width), :]), nt(kv, w_v[b, pl.ds(width, width), :])

    def middle(scores, dprobs, b, l_of, keep):
        dl = drow[b]
        ps, ds = [], []
        for k in range(scores.shape[0] // BLOCK):
            rows = slice(k * BLOCK, (k + 1) * BLOCK)
            p = jnp.exp2(scores[rows] * LOG2E - l_of(k))
            if keep is not None:
                p = jnp.where(keep, p, 0.0)
            ps.append(p.astype(BF16))
            ds.append((p * (dprobs[rows] - dl)).astype(BF16))
        return jnp.concatenate([jnp.concatenate(ds, axis=0), jnp.concatenate(ps, axis=0)], axis=1)

    def second(kv, b, dp):
        return nn(dp, w_v[b]), tn(kv[:, :DH], dp[:, :width])

    def tile(kv, b, l_of, keep):
        return second(kv, b, middle(*first(kv, b), b, l_of, keep))

    keep = lax.broadcasted_iota(jnp.int32, (BLOCK, width), 0) <= lax.rem(
        lax.broadcasted_iota(jnp.int32, (BLOCK, width), 1), BLOCK
    )
    for b in range(nb):
        rows = pl.ds(b * BLOCK, BLOCK)
        dkv, dq = tile(kv_v[rows, :], b, lambda k: lrow[b], keep)
        dkv_own[rows, :] = dkv
        dqt[b] = dq

    @pl.when(x != 0)
    def _():
        for cp in x_out:
            cp.start()

    def arrived(l):
        @pl.when(gets_from[l])
        def _():
            taken(far.at[l], kv_r.at[l])

    arrived(1)
    pass_on(2)

    def terms(l):
        kv = far[l]
        raw = [first(kv, b) for b in range(nb)]
        dps = [middle(*raw[b], b, lambda k, b=b: nrow[l, b, k], None) for b in range(nb)]
        for b in range(nb):
            dqt[b] = dqt[b] + tn(kv[:, :DH], dps[b][:, :width])
        return jnp.concatenate(dps, axis=1)

    def toward_keys(l, dps):
        back[l] = nn(dps, w_v[...].reshape(nb * 2 * width, 2 * DH)).astype(BF16)

    def level(l):
        toward_keys(l, terms(l))

    ret_out = [remote(back.at[l], ret.at[l], r_s, r_r, segment(me - reach[l])) for l in range(LEVELS)]

    def run_level(l):
        @pl.when(gets_from[l])
        def _():
            level(l)

    def give_back(l):
        @pl.when(gets_from[l])
        def _():
            ret_out[l].start()

    def flip(b):
        for k in range(step):
            xt[b * step + k] = xg[b, :, pl.ds(k * 128, 128)].T

    def block_of_x(b):
        @pl.when(x != b)
        def _():
            taken(xg.at[b], x_r.at[b])

        flip(b)

    run_level(1)
    arrived(0)
    run_level(0)
    arrived(2)

    @pl.when(goes[3])
    def _():
        pl.semaphore_wait(near_sem.at[0], 1)
        kv_out[3].start()
        hello(near_sem.at[0], zmate(-step))

    give_back(1)
    give_back(0)
    run_level(2)
    give_back(2)

    arrived(3)

    @pl.when(late)
    def _():
        dp_v[...] = terms(3)

    @pl.when(goes[5])
    def _():
        pl.semaphore_wait(near_sem.at[1], 1)
        taken(far.at[4], kv_r.at[3])
        kv_out[5].start()

    block_of_x(0)

    for b in range(nb):
        t = (dqt[b] * (DH**-0.5)).astype(BF16).T
        for h in range(heads):
            dq_ref[pl.ds(b * BLOCK, BLOCK), pl.ds(h * DH, DH)] = t[h * BLOCK : (h + 1) * BLOCK]
    dq = dq_ref[...]

    feats = 128

    def product(z0, n):
        return nn(xt[pl.ds(z0, n)].reshape(n * feats, tok), dq)

    def rows_of(g):
        z0, n = groups[g]
        return pl.ds(z0, n)

    def pair(g):
        z0, n = groups[g]

        def one(i, carry):
            part = product(z0 + i, 1).reshape(ny, nc, feats // seats, width).astype(BF16)
            for e in range(nc):
                pe[e, z0 + i] = part[:, e]
            return carry

        lax.fori_loop(0, n, one, 0, unroll=n <= 2)
        rows = rows_of(g)
        remote(pe.at[1 - c, rows], pr.at[rows], p_s, p_r.at[g], at(z, y, 1 - c, x)).start()

    def across_y(g):
        rows = rows_of(g)
        taken(pr.at[rows], p_r.at[g])
        for yy in range(ny):
            ys[yy, rows] = (pe[c, rows, yy].astype(F32) + pr[rows, yy].astype(F32)).astype(BF16)
        yr[y, rows] = ys[y, rows]
        for d in sorted(range(1, ny), key=lambda d: -min(d, ny - d)):
            yy = lax.rem(y + d, ny)
            remote(ys.at[yy, rows], yr.at[y, rows], y_s, y_r.at[g], at(z, yy, c, x)).start()

    def to_owner(zz):
        @pl.when(zz != z)
        def _():
            remote(zs.at[zz], zr.at[z], z_s, z_r, at(zz, y, c, x)).start()

        @pl.when(zz == z)
        def _():
            zr[z] = zs[zz]

    def across_z(g):
        z0, n = groups[g]
        rows = rows_of(g)
        taken(yr.at[pl.ds(0, ny - 1), rows], y_r.at[g])
        for i in range(n):
            acc = yr[0, z0 + i].astype(F32)
            for k in range(1, ny):
                acc = acc + yr[k, z0 + i].astype(F32)
            zs[z0 + i] = acc.astype(BF16)
            to_owner(z0 + i)

    @pl.when(jnp.logical_not(late))
    def _():
        pair(0)
        pl.semaphore_wait(near_sem.at[3], 2)
        across_y(0)
        pair(1)
        across_y(1)
        block_of_x(1)
        block_of_x(2)
        block_of_x(3)
        pair(3)
        across_y(3)

        @pl.when(goes[5])
        def _():
            pl.semaphore_wait(near_sem.at[0], 1)

            @pl.when(z == 0)
            def _():
                pl.semaphore_wait(near_sem.at[2], 1)

            hello(near_sem.at[1], zmate(step))

        @pl.when(goes[3])
        def _():
            pl.semaphore_wait(near_sem.at[1], 1)
            hello(near_sem.at[1], zmate(step))

        pair(2)
        across_y(2)
        across_z(0)
        across_z(1)
        across_z(2)
        across_z(3)

    @pl.when(late)
    def _():
        pair(0)
        pair(1)
        pl.semaphore_wait(near_sem.at[3], 2)
        across_y(0)
        across_y(1)
        toward_keys(3, dp_v[...])
        ret_out[3].start()
        block_of_x(1)
        pair(2)
        across_y(2)
        block_of_x(2)
        block_of_x(3)
        pair(3)

        @pl.when(z < last)
        def _():
            pl.semaphore_wait(near_sem.at[1], 1)

        @pl.when(z == last)
        def _():
            pl.semaphore_wait(near_sem.at[2], 1)

        across_z(0)
        across_z(1)
        across_y(3)
        across_z(2)

    def count(flags):
        return sum(f.astype(jnp.int32) for f in flags)

    def slots(ref, sem, number, most):
        for k in range(1, most + 1):

            @pl.when(number == k)
            def _(k=k):
                taken(ref.at[pl.ds(0, k)], sem)

    slots(ret, r_r, count(sends_to), LEVELS)
    for l in range(LEVELS):

        @pl.when(sends_to[l])
        def _(l=l):
            dkv_own[...] = dkv_own[...] + ret[l].astype(F32)

    total_kv = dkv_own[...].T
    dk_ref[...] = total_kv[:DH].astype(BF16)
    dv_ref[...] = total_kv[DH:].astype(BF16)

    @pl.when(late)
    def _():
        across_z(ng - 1)

    slots(far, kv_s, count(goes), LEVELS + 1)
    slots(back, r_s, count(gets_from), LEVELS)
    taken(xg.at[pl.ds(0, nx - 1)], x_s)
    taken(pr, p_s)
    taken(ys.at[pl.ds(0, ny - 1)], y_s)
    taken(zs.at[pl.ds(0, nz - 1)], z_s)
    taken(zr.at[pl.ds(0, nz - 1)], z_r)
    acc = zr[0].astype(F32)
    for k in range(1, nz):
        acc = acc + zr[k].astype(F32)
    dw_ref[...] = acc


def write(dq, dk, dv, dw, dq_out, dk_out, dv_out, dw_out, sem):
    copies = [
        pltpu.make_async_copy(s, d, sem.at[i])
        for i, (s, d) in enumerate(((dq, dq_out), (dk, dk_out), (dv, dv_out), (dw, dw_out)))
    ]
    for cp in copies:
        cp.start()
    for cp in copies:
        cp.wait()


def shards(layer_input, queries, keys, values, attn_out, grad_out, log_sum, chosen):
    nz, ny, nc, nx = (SIZES[a] for a in ("z", "y", "c", "x"))
    total = nz * ny * nc
    tok, qw = queries.shape
    nb = tok // BLOCK
    heads = qw // DH
    feats = layer_input.shape[1]
    rows_out = feats * nx // total
    groups = groups_of(nz)
    ng = len(groups)
    dma = pltpu.SemaphoreType.DMA
    vm = pltpu.VMEM
    hbm = pl.BlockSpec(memory_space=pltpu.HBM)
    vmem = pl.BlockSpec(memory_space=pltpu.VMEM)
    shapes = (
        jax.ShapeDtypeStruct((tok, qw), BF16),
        jax.ShapeDtypeStruct((DH, tok), BF16),
        jax.ShapeDtypeStruct((DH, tok), BF16),
        jax.ShapeDtypeStruct((rows_out, qw), F32),
    )
    parts = pl.pallas_call(
        kernel,
        out_shape=tuple(pltpu.VMEM(s.shape, s.dtype) for s in shapes),
        in_specs=[hbm] * 8,
        out_specs=(vmem,) * 4,
        scratch_shapes=[
            vm((3, tok, qw), BF16), vm((heads, tok), F32), vm((LEVELS * PER, chosen.shape[0]), jnp.int32),
            vm((2, DH, tok), BF16), vm((tok, 2 * DH), BF16),
            vm((nb, 2 * heads * BLOCK, 2 * DH), BF16), vm((tok, nb * 2 * heads * BLOCK), BF16),
            vm((nb, 1, heads * BLOCK), F32),
            vm((LEVELS, nb, nb, 1, heads * BLOCK), F32), vm((nb, 1, heads * BLOCK), F32),
            vm((nb, DH, heads * BLOCK), F32), vm((tok, 2 * DH), F32),
            vm((LEVELS + 1, tok, 2 * DH), BF16), vm((LEVELS, tok, 2 * DH), BF16), vm((LEVELS, tok, 2 * DH), BF16),
            vm((nx, tok, feats), BF16), vm((nz, feats * nx // nz, tok), BF16),
            vm((nc, nz, ny, rows_out, qw), BF16), vm((nz, ny, rows_out, qw), BF16),
            vm((ny, nz, rows_out, qw), BF16), vm((ny, nz, rows_out, qw), BF16),
            vm((nz, rows_out, qw), BF16), vm((nz, rows_out, qw), BF16),
            dma((6,)), dma((LEVELS,)), dma((nx,)), dma, dma((ng,)), dma((ng,)), dma,
            pltpu.SemaphoreType.REGULAR((4,)),
        ],
        compiler_params=pltpu.CompilerParams(collective_id=0, has_side_effects=True, vmem_limit_bytes=48 * 1024 * 1024),
        name="whole",
    )(
        *(
            pltpu.with_memory_space_constraint(a, pltpu.HBM)
            for a in (layer_input, queries, keys.T, values.T, attn_out, grad_out, log_sum.T, chosen.T)
        )
    )
    parts = [pltpu.with_memory_space_constraint(a, pltpu.VMEM) for a in parts]
    dq, dk, dv, dw = pl.pallas_call(
        write,
        out_shape=shapes,
        in_specs=[vmem] * 4,
        out_specs=(hbm,) * 4,
        scratch_shapes=[dma((4,))],
        name="write",
    )(*parts)
    return dq, dk.T, dv.T, dw


def solution(mesh):
    torus = Mesh(
        mesh.devices.reshape(SIZES["z"], SIZES["y"], SIZES["c"], SIZES["x"]), ("z", "y", "c", "x")
    )
    spec = P(KV, "x")
    return jax.shard_map(
        shards,
        mesh=torus,
        in_specs=(spec,) * 7 + (P(),),
        out_specs=(spec,) * 4,
        check_vma=False,
    )
```
